128 devices in a mesh: fs: 16 (over z, y), tp: 8 (over x, core).
Axes of the slice: x: 4, y: 4, z: 4, core: 2. Of those that a mesh axis runs over, the one named last changes fastest.
Arguments:
- layer_input: bfloat16 [12288, 2048], P('fs', 'tp'), may hold values from -6 to 6
- out_cotangent: bfloat16 [12288, 2048], P('fs', 'tp'), may hold values from -6 to 6
- gate_matrix: bfloat16 [2048, 6144], P('fs', 'tp'), may hold values from -0.125 to 0.125
- up_matrix: bfloat16 [2048, 6144], P('fs', 'tp'), may hold values from -0.125 to 0.125
- down_matrix: bfloat16 [6144, 2048], P('tp', 'fs'), may hold values from -0.078125 to 0.078125
Outputs:
- input_grad: bfloat16 [12288, 2048], P('fs', 'tp')
- gate_grad: float32 [2048, 6144], P('fs', 'tp')
- up_grad: float32 [2048, 6144], P('fs', 'tp')
- down_grad: float32 [6144, 2048], P('tp', 'fs')
The draws below stay inside these ranges and needn't reach their ends.
All inputs are finite; a program needn't handle non-finite values.
Results may differ from the reference program's by a relative error of at most 0.014.
Values may be sent and summed in bfloat16 or wider, within the bound.
A program may use at most 128 MiB of HBM per device.

```python
import jax
import jax.numpy as jnp

D = 2048
FF = 6144
TOKENS = 12288
N_TP = 8


def raised(array, key, source, target, parts, factor):
    def block_of(dim):
        return (jnp.arange(array.shape[dim]) // (array.shape[dim] // parts)).reshape((-1,) + (1,) * (array.ndim - 1 - dim))

    one_side = jax.random.permutation(key, parts)[block_of(target)]
    other_side = (block_of(target) + parts // 2) % parts
    return jnp.where((block_of(source) == one_side) | (block_of(source) == other_side), factor * array, array)


def levels(stream_key, shape, split, least, largest):
    factor_of = 1.0
    for dim, shards_of in split:
        heights = jax.random.uniform(jax.random.fold_in(jax.random.fold_in(stream_key, 6), dim), (shards_of,), jnp.float32, least / len(split), largest / len(split))
        factor_of = factor_of * jnp.repeat(jnp.exp(heights), shape[dim] // shards_of).reshape((-1,) + (1,) * (len(shape) - 1 - dim))
    return factor_of


def gaussian(own_key, shape, scale, limit, split=(), kind=jnp.bfloat16):
    result = scale * jax.random.normal(own_key, shape, jnp.float32)
    if split:
        result = result * levels(own_key, shape, split, -0.22, 0.18)
    return jnp.clip(result, -limit, limit).astype(kind)


def noise_with(key, extent, spread, most, pieces, heavy, held_as=jnp.bfloat16):
    values = spread * jax.random.normal(key, extent, jnp.float32)
    if pieces:
        values = values * levels(key, extent, pieces, -0.22, 0.18)
    return jnp.clip(raised(values, jax.random.fold_in(key, 3), *heavy), -most, most).astype(held_as)


def setup_inputs(seed: int = 0) -> dict:
    key_of = jax.random.split(jax.random.key(seed), 6)
    layer_input = gaussian(key_of[0], (TOKENS, D), 1.0, 6.0, ((0, 16), (1, 8)))
    out_cotangent = noise_with(key_of[1], (TOKENS, D), 1.0, 6.0, ((0, 16), (1, 8)), (0, 1, 16, 2.0))
    gate_matrix = gaussian(key_of[2], (D, FF), D ** -0.5, 0.125, ((0, 16), (1, 8)))
    up_matrix = gaussian(key_of[3], (D, FF), D ** -0.5, 0.125, ((0, 16), (1, 8)))
    down_matrix = gaussian(key_of[4], (FF, D), FF ** -0.5, 0.078125, ((0, 8), (1, 16)))
    return dict(layer_input=layer_input, out_cotangent=out_cotangent, gate_matrix=gate_matrix, up_matrix=up_matrix, down_matrix=down_matrix)


def reference(layer_input, out_cotangent, gate_matrix, up_matrix, down_matrix):
    gate_pre = jnp.dot(layer_input, gate_matrix, preferred_element_type=jnp.float32)
    up_pre = jnp.dot(layer_input, up_matrix, preferred_element_type=jnp.float32)
    sigmoid_gate = jax.nn.sigmoid(gate_pre)
    activation = gate_pre * sigmoid_gate
    hidden = (activation * up_pre).astype(jnp.bfloat16)
    hidden_delta = jnp.dot(out_cotangent, down_matrix.T, preferred_element_type=jnp.float32)
    up_delta = (hidden_delta * activation).astype(jnp.bfloat16)
    gate_delta = (hidden_delta * up_pre * sigmoid_gate * (1.0 + gate_pre * (1.0 - sigmoid_gate))).astype(jnp.bfloat16)
    gate_grad = jnp.dot(layer_input.T, gate_delta, preferred_element_type=jnp.float32)
    up_grad = jnp.dot(layer_input.T, up_delta, preferred_element_type=jnp.float32)
    down_grad = jnp.dot(hidden.T, out_cotangent, preferred_element_type=jnp.float32)
    block_width = FF // N_TP
    summed = jnp.zeros(layer_input.shape, jnp.float32)
    for block_index in range(N_TP):
        first_col = block_index * block_width
        last_col = first_col + block_width
        partial_value = jnp.dot(gate_delta[:, first_col:last_col], gate_matrix[:, first_col:last_col].T, preferred_element_type=jnp.float32)
        partial_value = partial_value + jnp.dot(up_delta[:, first_col:last_col], up_matrix[:, first_col:last_col].T, preferred_element_type=jnp.float32)
        summed = summed + partial_value.astype(jnp.bfloat16).astype(jnp.float32)
    return summed.astype(jnp.bfloat16), gate_grad, up_grad, down_grad
```

```python
import jax
import jax.numpy as jnp
from jax import lax
from jax.experimental import pallas as pl
from jax.experimental.pallas import tpu as pltpu
from jax.sharding import PartitionSpec as P

MESH = pl.DeviceIdType.MESH
BF = jnp.bfloat16
F32 = jnp.float32
SIDE = 4
ORDER = (2, 1, -1, 0)


def kernel_of(rows, tokens, width, hidden):
    cols = 3 * hidden // 2
    half = rows // 2
    feats = width // 8
    band = SIDE * rows
    halftok = tokens // 2

    def kernel(x_in, q_in, gate_in, up_in, down_in, dx_out, gate_out, up_out, down_out,
               W, XQ, ACC, D, G, R1, R2, R3, R4, PD, E0, E1, E2, DN, load_sem, ss, rs):
        fs, tp = lax.axis_index("fs"), lax.axis_index("tp")
        z, y = fs // SIDE, fs % SIDE
        x, c = tp // 2, tp % 2

        def turn(a, o):
            return (a + (o % SIDE)) % SIDE

        def fs_dev(f):
            return {"fs": f, "tp": tp}

        def tp_dev(t):
            return {"fs": fs, "tp": t}

        mine = pl.ds(pl.multiple_of(fs * rows, rows), rows)
        my_feats = pl.ds(pl.multiple_of(tp * feats, feats), feats)
        loads = [
            pltpu.make_async_copy(down_in, DN, load_sem.at[0]),
            pltpu.make_async_copy(gate_in, W.at[mine, 0:hidden], load_sem.at[1]),
            pltpu.make_async_copy(up_in, W.at[mine, hidden : 2 * hidden], load_sem.at[2]),
            pltpu.make_async_copy(x_in, XQ.at[0:tokens, my_feats], load_sem.at[3]),
            pltpu.make_async_copy(q_in, XQ.at[tokens : 2 * tokens, my_feats], load_sem.at[4]),
        ]
        for load in loads:
            load.start()

        def big_dev(k, d):
            return fs_dev(turn(z, d) * SIDE + y) if k == 0 else fs_dev(z * SIDE + turn(y, d))

        def small_dev(k, d):
            return big_dev(1 - k, d)

        sibling = tp_dev(x * 2 + (1 - c))

        def x_dev(d):
            return tp_dev(turn(x, d) * 2 + c)

        barrier = pltpu.get_barrier_semaphore()
        for partner in (big_dev(0, 1), big_dev(0, -1), big_dev(1, 1), big_dev(1, -1),
                        x_dev(1), x_dev(-1), sibling):
            pl.semaphore_signal(barrier, inc=1, device_id=partner, device_id_type=MESH)
        loads[0].wait()
        W[mine, 2 * hidden : 3 * hidden] = DN[...].astype(F32).T.astype(BF)
        for load in loads[1:]:
            load.wait()
        pl.semaphore_wait(barrier, 7)

        slots, sent = {}, []

        def slot(name):
            if name not in slots:
                slots[name] = len(slots)
            return slots[name]

        def send(name, src, dst, dev):
            n = slot(name)
            copy = pltpu.make_async_remote_copy(
                src_ref=src, dst_ref=dst, send_sem=ss.at[n], recv_sem=rs.at[n],
                device_id=dev, device_id_type=MESH)
            copy.start()
            sent.append(copy)

        def arrived(name, dst):
            n = slot(name)
            pltpu.make_async_remote_copy(
                src_ref=dst, dst_ref=dst, send_sem=ss.at[n], recv_sem=rs.at[n],
                device_id=sibling, device_id_type=MESH).wait_recv()

        def block(k, so, bo, part=None):
            zo, yo = (bo, so) if k == 0 else (so, bo)
            start = (turn(z, zo) * SIDE + turn(y, yo)) * rows
            if part is None:
                return pl.ds(pl.multiple_of(start, rows), rows)
            return pl.ds(pl.multiple_of(start + part * half, half), half)

        def lanes(k):
            return slice(k * cols, (k + 1) * cols)

        def w(k, so, bo, part=None):
            return W.at[block(k, so, bo, part), lanes(k)]

        def near(k):
            for d in (1, -1):
                send(("a1", k, d), w(k, 0, 0), w(k, 0, 0), small_dev(k, d))

        def far(k, r):
            for d in (1, -1):
                send(("a3", k, r, d), w(k, r, 0), w(k, r, 0), big_dev(k, d))

        def near_arrived(k):
            for d in (1, -1):
                arrived(("a1", k, d), w(k, -d, 0))
                part = 0 if d == 1 else 1
                send(("a2", k, d), w(k, -d, 0, part), w(k, -d, 0, part), small_dev(k, d))

        def opposite_arrived(k):
            for d in (1, -1):
                arrived(("a2", k, d), w(k, 2, 0, 0 if d == 1 else 1))

        def far_arrived(k, r):
            for d in (1, -1):
                arrived(("a3", k, r, d), w(k, r, -d))
                part = 0 if d == 1 else 1
                send(("a4", k, r, d), w(k, r, -d, part), w(k, r, -d, part), big_dev(k, d))

        def last_arrived(k, r):
            for d in (1, -1):
                arrived(("a4", k, r, d), w(k, r, 2, 0 if d == 1 else 1))

        def xq(xo, core, part=None):
            start = (turn(x, xo) * 2 + core) * feats
            lane = pl.ds(pl.multiple_of(start, feats), feats)
            if part is None:
                return XQ.at[:, lane]
            return XQ.at[part * tokens : (part + 1) * tokens, lane]

        near(0)
        near(1)
        for d in (1, -1):
            send(("x1", d), xq(0, c), xq(0, c), x_dev(d))
        far(0, 0)
        far(1, 0)
        send("s0", xq(0, c), xq(0, c), sibling)

        near_arrived(0)
        near_arrived(1)
        for r in (1, -1):
            far(0, r)
            far(1, r)
        far_arrived(0, 0)
        far_arrived(1, 0)
        opposite_arrived(0)
        far(0, 2)
        opposite_arrived(1)
        far(1, 2)

        for d in (1, -1):
            arrived(("x1", d), xq(-d, c))
            part = 0 if d == 1 else 1
            send(("x2", d), xq(-d, c, part), xq(-d, c, part), x_dev(d))
        for d in (1, -1):
            send(("s1", d), xq(-d, c), xq(-d, c), sibling)
        far_arrived(0, 1)
        far_arrived(1, 1)
        for d in (1, -1):
            part = 0 if d == 1 else 1
            arrived(("x2", d), xq(2, c, part))
            send(("s2", d), xq(2, c, part), xq(2, c, part), sibling)
        far_arrived(0, -1)
        far_arrived(1, -1)
        arrived("s0", xq(0, 1 - c))
        for d in (1, -1):
            arrived(("s1", d), xq(-d, 1 - c))
        for d in (1, -1):
            arrived(("s2", d), xq(2, 1 - c, 0 if d == 1 else 1))

        tile = tokens // 3

        def dot(a, b, dims):
            return lax.dot_general(a, b, (dims, ((), ())), preferred_element_type=F32)

        def put(at, lane, value, first):
            if first:
                ACC[at, lane] = value
            else:
                ACC[at, lane] += value

        def forward(k, o, first=False):
            def piece(m, carry):
                at = pl.ds(pl.multiple_of(m * tile, tile), tile)
                low = pl.ds(pl.multiple_of(tokens + m * tile, tile), tile)
                if k == 0:
                    span = pl.ds(pl.multiple_of(turn(z, o) * band, band), band)
                    put(at, slice(0, cols),
                        dot(XQ[at, span], W[span, 0:cols], ((1,), (0,))), first)
                else:
                    spans = [pl.ds(pl.multiple_of(i * band + turn(y, o) * rows, rows), rows)
                             for i in range(SIDE)]
                    a = jnp.concatenate([XQ[at, s] for s in spans], axis=1)
                    b = jnp.concatenate([W[s, cols : 2 * hidden] for s in spans], axis=0)
                    put(at, slice(cols, 2 * hidden), dot(a, b, ((1,), (0,))), first)
                    a = jnp.concatenate([XQ[low, s] for s in spans], axis=1)
                    b = jnp.concatenate([W[s, 2 * hidden : 3 * hidden] for s in spans], axis=0)
                    put(at, slice(2 * hidden, 3 * hidden), dot(a, b, ((1,), (0,))), first)
                return carry
            lax.fori_loop(0, 3, piece, 0)

        forward(0, 0, True)
        forward(1, 0, True)
        far_arrived(0, 2)
        far_arrived(1, 2)
        for o in (1, -1):
            forward(0, o)
            forward(1, o)
        for k in (0, 1):
            for r in (0, 1, -1, 2):
                last_arrived(k, r)
            forward(k, 2)

        step = tokens // 24

        def gate(m, carry):
            at = pl.ds(pl.multiple_of(m * step, step), step)
            g = ACC[at, 0:hidden]
            u = ACC[at, hidden : 2 * hidden]
            e = ACC[at, 2 * hidden : 3 * hidden]
            s = jax.nn.sigmoid(g)
            act = g * s
            D[at, 0:hidden] = (e * u * s * (1.0 + g * (1.0 - s))).astype(BF)
            D[at, hidden : 2 * hidden] = (e * act).astype(BF)
            D[at, 2 * hidden : 3 * hidden] = (act * u).astype(BF)
            return carry

        lax.fori_loop(0, 24, gate, 0)

        def grads(k, o):
            def piece(p, carry):
                if k == 0:
                    span = pl.ds(pl.multiple_of(turn(z, o) * band + p * 2 * rows, 2 * rows), 2 * rows)
                    G[span, 0:cols] = dot(
                        XQ[0:tokens, span], D[:, 0:cols], ((0,), (0,))).astype(BF)
                else:
                    spans = [pl.ds(pl.multiple_of((2 * p + i) * band + turn(y, o) * rows, rows), rows)
                             for i in range(2)]
                    a = jnp.concatenate([XQ[0:tokens, s] for s in spans], axis=1)
                    r = dot(a, D[:, cols : 2 * hidden], ((0,), (0,))).astype(BF)
                    a = jnp.concatenate([XQ[tokens : 2 * tokens, s] for s in spans], axis=1)
                    t = dot(a, D[:, 2 * hidden : 3 * hidden], ((0,), (0,))).astype(BF)
                    for i in range(2):
                        G[spans[i], cols : 2 * hidden] = r[i * rows : (i + 1) * rows]
                        G[spans[i], 2 * hidden : 3 * hidden] = t[i * rows : (i + 1) * rows]
                return carry
            lax.fori_loop(0, 2, piece, 0)

        def g(k, so, bo, part=None):
            return G.at[block(k, so, bo, part), lanes(k)]

        def add_into(ref, *others):
            def piece(m, carry):
                at = pl.ds(pl.multiple_of(m * 16, 16), 16)
                total = ref[at, :].astype(F32)
                for other in others:
                    total = total + other[at, :].astype(F32)
                ref[at, :] = total.astype(BF)
                return carry
            lax.fori_loop(0, ref.shape[0] // 16, piece, 0)

        def s1(k):
            for j, r in enumerate(ORDER):
                for i, d in enumerate((1, -1)):
                    send(("g1", k, j, d), g(k, r, 2, i), R1.at[k, i, j], big_dev(k, d))

        def s2(k, j):
            r = ORDER[j]
            for i, d in enumerate((1, -1)):
                arrived(("g1", k, j, d), R1.at[k, i, j])
                add_into(g(k, r, d, i), R1.at[k, i, j])
            for i, d in enumerate((1, -1)):
                send(("g2", k, j, d), g(k, r, d), R2.at[k, i, j], big_dev(k, d))

        def two(k, j):
            for i, d in enumerate((1, -1)):
                arrived(("g2", k, j, d), R2.at[k, i, j])

        def s3(k):
            two(k, 0)
            add_into(g(k, 2, 0), R2.at[k, 0, 0], R2.at[k, 1, 0])
            for i, d in enumerate((1, -1)):
                send(("g3", k, d), g(k, 2, 0, i), R3.at[k, i], small_dev(k, d))

        def s4(k, i):
            d = (1, -1)[i]
            two(k, 1 + i)
            add_into(g(k, d, 0), R2.at[k, 0, 1 + i], R2.at[k, 1, 1 + i])
            arrived(("g3", k, d), R3.at[k, i])
            add_into(g(k, d, 0, i), R3.at[k, i])
            send(("g4", k, d), g(k, d, 0), R4.at[k, i], small_dev(k, d))

        def partial_of(xo, core):
            start = (turn(x, xo) * 2 + core) * feats
            span = pl.ds(pl.multiple_of(start, feats), feats)

            def piece(m, carry):
                at = pl.ds(pl.multiple_of(m * tile, tile), tile)
                PD[at, span] = dot(
                    D[at, 0 : 2 * hidden], W[span, 0 : 2 * hidden], ((1,), (1,))).astype(BF)
                return carry
            lax.fori_loop(0, 3, piece, 0)

        def pd(xo, core, part=None):
            start = (turn(x, xo) * 2 + core) * feats
            lane = pl.ds(pl.multiple_of(start, feats), feats)
            if part is None:
                return PD.at[:, lane]
            return PD.at[part * halftok : (part + 1) * halftok, lane]

        grads(0, 2)
        s1(0)
        grads(1, 2)
        s1(1)
        for o in (1, -1):
            grads(0, o)
            grads(1, o)
        for j in (0, 1, 2):
            s2(0, j)
            s2(1, j)
        for j, r in enumerate(ORDER):
            partial_of(r, 1 - c)
            send(("d0", j), pd(r, 1 - c), E0.at[j], sibling)
        for r in ORDER:
            partial_of(r, c)
        arrived(("d0", 0), E0.at[0])
        add_into(pd(2, c), E0.at[0])
        for i, d in enumerate((1, -1)):
            send(("d1", d), pd(2, c, i), E1.at[i], x_dev(d))
        grads(0, 0)
        grads(1, 0)
        for j in (1, 2):
            arrived(("d0", j), E0.at[j])
            add_into(pd(ORDER[j], c), E0.at[j])
        s3(0)
        s3(1)
        s2(0, 3)
        s2(1, 3)
        for i, d in enumerate((1, -1)):
            arrived(("d1", d), E1.at[i])
            add_into(pd(d, c, i), E1.at[i])
            send(("d2", d), pd(d, c), E2.at[i], x_dev(d))
        for i in (0, 1):
            s4(0, i)
            s4(1, i)
        arrived(("d0", 3), E0.at[3])
        for i, d in enumerate((1, -1)):
            arrived(("d2", d), E2.at[i])

        own = pd(0, c)

        def last_dx(m, carry):
            at = pl.ds(pl.multiple_of(m * 16, 16), 16)
            total = (own[at, :].astype(F32) + E0[3, at, :].astype(F32)
                     + E2[0, at, :].astype(F32) + E2[1, at, :].astype(F32))
            dx_out[at, :] = total.astype(BF)
            return carry

        lax.fori_loop(0, tokens // 16, last_dx, 0)
        for k in (0, 1):
            two(k, 3)
            for i, d in enumerate((1, -1)):
                arrived(("g4", k, d), R4.at[k, i])
            base = g(k, 0, 0)

            def last_grad(m, carry):
                at = pl.ds(pl.multiple_of(m * 16, 16), 16)
                total = (base[at, :].astype(F32) + R2[k, 0, 3, at, :].astype(F32)
                         + R2[k, 1, 3, at, :].astype(F32) + R4[k, 0, at, :].astype(F32)
                         + R4[k, 1, at, :].astype(F32))
                rest = cols - hidden
                if k == 0:
                    gate_out[at, :] = total[:, 0:hidden]
                    up_out[at, 0:rest] = total[:, hidden:cols]
                else:
                    up_out[at, rest:hidden] = total[:, 0:rest]
                    down_out[at, :] = total[:, rest:cols]
                return carry

            lax.fori_loop(0, rows // 16, last_grad, 0)
        for copy in sent:
            copy.wait_send()

    count = 2 * (2 + 2 + 8 + 8) + 9 + 2 * (8 + 8 + 2 + 2) + 4 + 2 + 2
    scratch = [
        pltpu.VMEM((width, 2 * cols), BF),
        pltpu.VMEM((2 * tokens, width), BF),
        pltpu.VMEM((tokens, 2 * cols), F32),
        pltpu.VMEM((tokens, 2 * cols), BF),
        pltpu.VMEM((width, 2 * cols), BF),
        pltpu.VMEM((2, 2, SIDE, half, cols), BF),
        pltpu.VMEM((2, 2, SIDE, rows, cols), BF),
        pltpu.VMEM((2, 2, half, cols), BF),
        pltpu.VMEM((2, 2, rows, cols), BF),
        pltpu.VMEM((tokens, width), BF),
        pltpu.VMEM((SIDE, tokens, feats), BF),
        pltpu.VMEM((2, halftok, feats), BF),
        pltpu.VMEM((2, tokens, feats), BF),
        pltpu.VMEM((hidden, rows), BF),
        pltpu.SemaphoreType.DMA((5,)),
        pltpu.SemaphoreType.DMA((count,)),
        pltpu.SemaphoreType.DMA((count,)),
    ]
    return kernel, scratch


def solution(mesh):
    def on_device(layer_input, out_cotangent, gate_matrix, up_matrix, down_matrix):
        tokens, feats = layer_input.shape
        rows, hidden = gate_matrix.shape
        width = feats * mesh.shape["tp"]
        kernel, scratch = kernel_of(rows, tokens, width, hidden)
        flops = 2 * 8 * tokens * width * hidden
        dx, gate_grad, up_grad, down_grad = pl.pallas_call(
            kernel,
            out_shape=(
                jax.ShapeDtypeStruct((tokens, feats), BF),
                jax.ShapeDtypeStruct((rows, hidden), F32),
                jax.ShapeDtypeStruct((rows, hidden), F32),
                jax.ShapeDtypeStruct((rows, hidden), F32),
            ),
            in_specs=[pl.BlockSpec(memory_space=pl.ANY)] * 5,
            out_specs=[pl.BlockSpec(memory_space=pltpu.VMEM)] * 4,
            scratch_shapes=scratch,
            compiler_params=pltpu.CompilerParams(
                collective_id=0, has_side_effects=True, vmem_limit_bytes=66_000_000),
            cost_estimate=pl.CostEstimate(
                flops=flops, bytes_accessed=4 << 20, transcendentals=tokens * hidden),
        )(layer_input, out_cotangent, gate_matrix, up_matrix, down_matrix)
        return dx, gate_grad, up_grad, down_grad.T

    return jax.shard_map(
        on_device, mesh=mesh,
        in_specs=(P("fs", "tp"), P("fs", "tp"), P("fs", "tp"), P("fs", "tp"), P("tp", "fs")),
        out_specs=(P("fs", "tp"), P("fs", "tp"), P("fs", "tp"), P("tp", "fs")),
        check_vma=False)
```

```python
import jax
import jax.numpy as jnp
from jax import lax
from jax.experimental import pallas as pl
from jax.experimental.pallas import tpu as pltpu
from jax.sharding import PartitionSpec as P

MESH = pl.DeviceIdType.MESH
BF = jnp.bfloat16
F32 = jnp.float32
SIDE = 4
ORDER = (2, 1, -1, 0)


def shares(hidden):
    first = 2 * hidden // 3
    return (first, hidden - first), (0, 3 * first)


def kernel_of(rows, tokens, width, hidden):
    size, base = shares(hidden)
    half = rows // 2
    feats = width // 8
    band = SIDE * rows
    halftok = tokens // 2
    every = 3 * hidden

    def kernel(x_in, q_in, gate_in, up_in, down_in, dx_out, sum_out, late_out,
               W, XQ, ACC, D, G, R1a, R1b, R2a, R2b, R3a, R3b, R4a, PD, E0, E1, E2, DN, SUM, DX,
               load_sem, store_sem, ss, rs):
        R1, R2, R3, R4 = (R1a, R1b), (R2a, R2b), (R3a, R3b), (R4a, late_out)
        fs, tp = lax.axis_index("fs"), lax.axis_index("tp")
        z, y = fs // SIDE, fs % SIDE
        x, c = tp // 2, tp % 2

        def turn(a, o):
            return (a + (o % SIDE)) % SIDE

        def fs_dev(f):
            return {"fs": f, "tp": tp}

        def tp_dev(t):
            return {"fs": fs, "tp": t}

        def big_dev(k, d):
            return fs_dev(turn(z, d) * SIDE + y) if k == 0 else fs_dev(z * SIDE + turn(y, d))

        def small_dev(k, d):
            return big_dev(1 - k, d)

        sibling = tp_dev(x * 2 + (1 - c))

        def x_dev(d):
            return tp_dev(turn(x, d) * 2 + c)

        barrier = pltpu.get_barrier_semaphore()
        for partner in (big_dev(0, 1), big_dev(0, -1), big_dev(1, 1), big_dev(1, -1),
                        x_dev(1), x_dev(-1), sibling):
            pl.semaphore_signal(barrier, inc=1, device_id=partner, device_id_type=MESH)
        mine = pl.ds(pl.multiple_of(fs * rows, rows), rows)
        my_feats = pl.ds(pl.multiple_of(tp * feats, feats), feats)
        loads = [
            pltpu.make_async_copy(down_in, DN, load_sem.at[0]),
            pltpu.make_async_copy(x_in, XQ.at[0:tokens, my_feats], load_sem.at[1]),
            pltpu.make_async_copy(q_in, XQ.at[tokens : 2 * tokens, my_feats], load_sem.at[2]),
        ]
        for p in (0, 1):
            at, h, from_ = base[p], size[p], p * size[0]
            for i, ref in enumerate((gate_in, up_in)):
                loads.append(pltpu.make_async_copy(
                    ref.at[:, from_ : from_ + h], W.at[mine, at + i * h : at + (i + 1) * h],
                    load_sem.at[len(loads)]))
        for load in loads:
            load.start()

        def load_in():
            loads[0].wait()
            turned = DN[...].astype(F32).T.astype(BF)
            for p in (0, 1):
                at, h, from_ = base[p], size[p], p * size[0]
                W[mine, at + 2 * h : at + 3 * h] = turned[:, from_ : from_ + h]
            for load in loads[1:]:
                load.wait()

        load_in()

        def meet():
            pl.semaphore_wait(barrier, 7)

        meet()

        slots = {}

        def slot(name):
            if name not in slots:
                slots[name] = len(slots)
            return slots[name]

        def send(group, name, src, dst, dev):
            pltpu.make_async_remote_copy(
                src_ref=src, dst_ref=dst, send_sem=ss.at[group], recv_sem=rs.at[slot(name)],
                device_id=dev, device_id_type=MESH).start()

        def awaited(name, like):
            return pltpu.make_async_remote_copy(
                src_ref=like, dst_ref=like, send_sem=ss.at[0], recv_sem=rs.at[slot(name)],
                device_id=sibling, device_id_type=MESH)

        def arrived(name, like):
            awaited(name, like).wait_recv()

        def left(group, like):
            pltpu.make_async_remote_copy(
                src_ref=like, dst_ref=like, send_sem=ss.at[group], recv_sem=rs.at[0],
                device_id=sibling, device_id_type=MESH).wait_send()

        def block(k, so, bo, part=None):
            zo, yo = (bo, so) if k == 0 else (so, bo)
            start = (turn(z, zo) * SIDE + turn(y, yo)) * rows
            if part is None:
                return pl.ds(pl.multiple_of(start, rows), rows)
            return pl.ds(pl.multiple_of(start + part * half, half), half)

        def lanes(p, k):
            cols = 3 * size[p] // 2
            return slice(base[p] + k * cols, base[p] + (k + 1) * cols)

        def blocks(ref, p, n):
            return ref.at[0 : n * rows, base[p] : base[p] + 3 * size[p]]

        def w(p, k, so, bo, part=None):
            return W.at[block(k, so, bo, part), lanes(p, k)]

        def near(p, k):
            for d in (1, -1):
                send(p, ("a1", p), w(p, k, 0, 0), w(p, k, 0, 0), small_dev(k, d))

        def far(p, r):
            for k in (0, 1):
                for d in (1, -1):
                    send(p, ("a3", p, r), w(p, k, r, 0), w(p, k, r, 0), big_dev(k, d))

        def near_arrived(p):
            arrived(("a1", p), blocks(W, p, 2))
            for k in (0, 1):
                for i, d in enumerate((1, -1)):
                    send(p, ("a2", p), w(p, k, -d, 0, i), w(p, k, -d, 0, i), small_dev(k, d))

        def opposite_arrived(p):
            arrived(("a2", p), blocks(W, p, 1))

        def far_arrived(p, r):
            arrived(("a3", p, r), blocks(W, p, 2))
            for k in (0, 1):
                for i, d in enumerate((1, -1)):
                    send(p, ("a4", p), w(p, k, r, -d, i), w(p, k, r, -d, i), big_dev(k, d))

        def last_arrived(p):
            arrived(("a4", p), blocks(W, p, 4))

        def xq(xo, core, part):
            start = (turn(x, xo) * 2 + core) * feats
            lane = pl.ds(pl.multiple_of(start, feats), feats)
            return XQ.at[part * tokens : (part + 1) * tokens, lane]

        def x_own(i):
            for d in (1, -1):
                part = i if d == 1 else 1 - i
                send(2, ("x1", i), xq(0, c, part), xq(0, c, part), x_dev(d))

        def to_sibling(xo, part):
            send(2, "sib", xq(xo, c, part), xq(xo, c, part), sibling)

        def x_first():
            arrived(("x1", 0), XQ.at[:, 0:feats])
            for i, d in enumerate((1, -1)):
                send(2, "x2", xq(-d, c, i), xq(-d, c, i), x_dev(d))
            for i, d in enumerate((1, -1)):
                to_sibling(-d, i)

        def x_second():
            arrived(("x1", 1), XQ.at[:, 0:feats])
            for i, d in enumerate((1, -1)):
                to_sibling(-d, 1 - i)

        def x_third():
            arrived("x2", XQ.at[:, 0:feats])
            for i in (0, 1):
                to_sibling(2, i)

        def x_last():
            arrived("sib", XQ.at[:, 0 : 4 * feats])

        near(0, 0)
        x_own(0)
        near(0, 1)
        far(0, 0)
        x_own(1)
        for part in (0, 1):
            to_sibling(0, part)
        for k in (0, 1):
            near(1, k)

        near_arrived(0)
        for r in (1, -1):
            far(0, r)
        x_first()
        far_arrived(0, 0)
        near_arrived(1)
        opposite_arrived(0)
        far(0, 2)
        far_arrived(0, 1)
        x_second()
        far_arrived(0, -1)
        far(1, 0)
        x_third()
        far_arrived(0, 2)
        for r in (1, -1):
            far(1, r)
        opposite_arrived(1)
        far(1, 2)
        x_last()

        tile = tokens // 3

        def dot(a, b, dims):
            return lax.dot_general(a, b, (dims, ((), ())), preferred_element_type=F32)

        def put(at, lane, value, first):
            if first:
                ACC[at, lane] = value
            else:
                ACC[at, lane] += value

        def forward(p, k, o, first=False):
            both = lanes(p, k)
            split = base[p] + 2 * size[p]

            def piece(m, carry):
                at = pl.ds(pl.multiple_of(m * tile, tile), tile)
                low = pl.ds(pl.multiple_of(tokens + m * tile, tile), tile)
                if k == 0:
                    span = pl.ds(pl.multiple_of(turn(z, o) * band, band), band)
                    put(at, both, dot(XQ[at, span], W[span, both], ((1,), (0,))), first)
                else:
                    spans = [pl.ds(pl.multiple_of(i * band + turn(y, o) * rows, rows), rows)
                             for i in range(SIDE)]
                    for top, lane in ((at, slice(both.start, split)), (low, slice(split, both.stop))):
                        a = jnp.concatenate([XQ[top, s] for s in spans], axis=1)
                        b = jnp.concatenate([W[s, lane] for s in spans], axis=0)
                        put(at, lane, dot(a, b, ((1,), (0,))), first)
                return carry
            lax.fori_loop(0, 3, piece, 0)

        step = tokens // 24

        def gate(p):
            h = size[p]
            one, two, three, four = (base[p] + i * h for i in range(4))

            def piece(m, carry):
                at = pl.ds(pl.multiple_of(m * step, step), step)
                g = ACC[at, one:two]
                u = ACC[at, two:three]
                e = ACC[at, three:four]
                s = jax.nn.sigmoid(g)
                act = g * s
                D[at, one:two] = (e * u * s * (1.0 + g * (1.0 - s))).astype(BF)
                D[at, two:three] = (e * act).astype(BF)
                D[at, three:four] = (act * u).astype(BF)
                return carry

            lax.fori_loop(0, 24, piece, 0)

        def grads(p, k, o):
            both = lanes(p, k)
            split = base[p] + 2 * size[p]

            def piece(n, carry):
                if k == 0:
                    span = pl.ds(pl.multiple_of(turn(z, o) * band + n * 2 * rows, 2 * rows), 2 * rows)
                    G[span, both] = dot(XQ[0:tokens, span], D[:, both], ((0,), (0,))).astype(BF)
                else:
                    spans = [pl.ds(pl.multiple_of((2 * n + i) * band + turn(y, o) * rows, rows), rows)
                             for i in range(2)]
                    for top, lane in ((0, slice(both.start, split)), (tokens, slice(split, both.stop))):
                        a = jnp.concatenate([XQ[top : top + tokens, s] for s in spans], axis=1)
                        r = dot(a, D[:, lane], ((0,), (0,))).astype(BF)
                        for i in range(2):
                            G[spans[i], lane] = r[i * rows : (i + 1) * rows]
                return carry
            lax.fori_loop(0, 2, piece, 0)

        def g(p, k, so, bo, part=None):
            return G.at[block(k, so, bo, part), lanes(p, k)]

        def add_into(ref, *others):
            def piece(m, carry):
                at = pl.ds(pl.multiple_of(m * 16, 16), 16)
                total = ref[at, :].astype(F32)
                for other in others:
                    total = total + other[at, :].astype(F32)
                ref[at, :] = total.astype(BF)
                return carry
            lax.fori_loop(0, ref.shape[0] // 16, piece, 0)

        def s1(p):
            for j, r in enumerate(ORDER):
                for k in (0, 1):
                    for i, d in enumerate((1, -1)):
                        send(3 + p, ("g1", p, j), g(p, k, r, 2, i), R1[p].at[k, i, j],
                             big_dev(k, d))

        def s2(p, j):
            r = ORDER[j]
            arrived(("g1", p, j), blocks(G, p, 1))
            for k in (0, 1):
                for i, d in enumerate((1, -1)):
                    add_into(g(p, k, r, d, i), R1[p].at[k, i, j])
            for k in (0, 1):
                for i, d in enumerate((1, -1)):
                    send(3 + p, ("g2", p, j), g(p, k, r, d), R2[p].at[k, i, j], big_dev(k, d))

        def two(p, j):
            arrived(("g2", p, j), blocks(G, p, 2))

        def s3(p):
            two(p, 0)
            for k in (0, 1):
                add_into(g(p, k, 2, 0), R2[p].at[k, 0, 0], R2[p].at[k, 1, 0])
            for k in (0, 1):
                for i, d in enumerate((1, -1)):
                    send(3 + p, ("g3", p), g(p, k, 2, 0, i), R3[p].at[k, i], small_dev(k, d))

        def pre4(p):
            for i, d in enumerate((1, -1)):
                two(p, 1 + i)
                for k in (0, 1):
                    add_into(g(p, k, d, 0), R2[p].at[k, 0, 1 + i], R2[p].at[k, 1, 1 + i])

        def s4(p):
            arrived(("g3", p), blocks(G, p, 1))
            for k in (0, 1):
                for i, d in enumerate((1, -1)):
                    add_into(g(p, k, d, 0, i), R3[p].at[k, i])
            for k in (0, 1):
                for i, d in enumerate((1, -1)):
                    send(3 + p, ("g4", p), g(p, k, d, 0), R4[p].at[k, i], small_dev(k, d))

        def keep(p, k, *others):
            own, to = g(p, k, 0, 0), SUM.at[:, lanes(p, k)]

            def piece(m, carry):
                at = pl.ds(pl.multiple_of(m * 16, 16), 16)
                total = own[at, :].astype(F32)
                for other in others:
                    total = total + other[at, :].astype(F32)
                to[at, :] = total
                return carry

            lax.fori_loop(0, rows // 16, piece, 0)

        def partial_of(xo, core):
            start = (turn(x, xo) * 2 + core) * feats
            span = pl.ds(pl.multiple_of(start, feats), feats)

            def piece(m, carry):
                at = pl.ds(pl.multiple_of(m * tile, tile), tile)
                total = 0.0
                for p in (0, 1):
                    lane = slice(base[p], base[p] + 2 * size[p])
                    total = total + dot(D[at, lane], W[span, lane], ((1,), (1,)))
                PD[at, span] = total.astype(BF)
                return carry
            lax.fori_loop(0, 3, piece, 0)

        def pd(xo, core, part=None):
            start = (turn(x, xo) * 2 + core) * feats
            lane = pl.ds(pl.multiple_of(start, feats), feats)
            if part is None:
                return PD.at[:, lane]
            return PD.at[part * halftok : (part + 1) * halftok, lane]

        for o in (0, 1, -1):
            for k in (0, 1):
                forward(0, k, o, o == 0)
        far_arrived(1, 0)
        last_arrived(0)
        for k in (0, 1):
            forward(0, k, 2)
        gate(0)
        far_arrived(1, 1)
        far_arrived(1, -1)
        for k in (0, 1):
            grads(0, k, 2)
        far_arrived(1, 2)
        s1(0)
        for o in (1, -1):
            for k in (0, 1):
                grads(0, k, o)

        for j, o in enumerate((0, 1, -1)):
            for k in (0, 1):
                forward(1, k, o, o == 0)
            s2(0, j)
        last_arrived(1)
        for k in (0, 1):
            forward(1, k, 2)
        gate(1)
        for k in (0, 1):
            grads(1, k, 2)
        s1(1)
        for o in (1, -1):
            for k in (0, 1):
                grads(1, k, o)
        for k in (0, 1):
            grads(0, k, 0)
        s3(0)
        s2(0, 3)
        for j, r in enumerate(ORDER):
            partial_of(r, 1 - c)
            send(5, ("d0", j), pd(r, 1 - c), E0.at[j], sibling)

        def sibling_sum(j):
            arrived(("d0", j), PD.at[:, 0:feats])
            add_into(pd(ORDER[j], c), E0.at[j])

        partial_of(2, c)
        sibling_sum(0)
        for i, d in enumerate((1, -1)):
            send(5, "d1", pd(2, c, i), E1.at[i], x_dev(d))
        for j in (1, 2):
            partial_of(ORDER[j], c)
            sibling_sum(j)
        for j in (0, 1, 2):
            s2(1, j)
        pre4(0)
        partial_of(0, c)
        s4(0)
        arrived("d1", PD.at[:, 0:feats])
        for i, d in enumerate((1, -1)):
            add_into(pd(d, c, i), E1.at[i])
            send(5, "d2", pd(d, c), E2.at[i], x_dev(d))
        for k in (0, 1):
            grads(1, k, 0)
        s3(1)
        s2(1, 3)
        pre4(1)

        stores = []

        def store(src, dst):
            copy = pltpu.make_async_copy(src, dst, store_sem.at[len(stores)])
            copy.start()
            stores.append(copy)

        def finish_dx():
            arrived(("d0", 3), PD.at[:, 0:feats])
            arrived("d2", PD.at[:, 0 : 2 * feats])
            own = pd(0, c)

            def piece(m, carry):
                at = pl.ds(pl.multiple_of(m * 16, 16), 16)
                total = (own[at, :].astype(F32) + E0[3, at, :].astype(F32)
                         + E2[0, at, :].astype(F32) + E2[1, at, :].astype(F32))
                DX[at, :] = total.astype(BF)
                return carry

            lax.fori_loop(0, tokens // 16, piece, 0)
            store(DX, dx_out)

        def finish_grads(p):
            two(p, 3)
            if p == 0:
                arrived(("g4", p), blocks(G, p, 2))
            for k in (0, 1):
                late = [R4[p].at[k, i] for i in (0, 1)] if p == 0 else []
                keep(p, k, R2[p].at[k, 0, 3], R2[p].at[k, 1, 3], *late)
            at = slice(base[p], base[p] + 3 * size[p])
            store(SUM.at[:, at], sum_out.at[:, at])

        finish_dx()
        s4(1)
        finish_grads(0)
        finish_grads(1)
        for p in (0, 1):
            left(p, blocks(W, p, 15))
            left(3 + p, blocks(G, p, 15))
        left(2, XQ.at[:, 0 : 7 * feats])
        left(5, PD.at[:, 0 : 7 * feats])
        for copy in stores:
            copy.wait()
        arrived(("g4", 1), blocks(G, 1, 2))

    count = 2 * (1 + 1 + 4 + 1) + 4 + 2 * (4 + 4 + 1 + 1) + 4 + 1 + 1
    n = [3 * h // 2 for h in size]
    scratch = [
        pltpu.VMEM((width, every), BF),
        pltpu.VMEM((2 * tokens, width), BF),
        pltpu.VMEM((tokens, every), F32),
        pltpu.VMEM((tokens, every), BF),
        pltpu.VMEM((width, every), BF),
        *[pltpu.VMEM((2, 2, SIDE, half, m), BF) for m in n],
        *[pltpu.VMEM((2, 2, SIDE, rows, m), BF) for m in n],
        *[pltpu.VMEM((2, 2, half, m), BF) for m in n],
        pltpu.VMEM((2, 2, rows, n[0]), BF),
        pltpu.VMEM((tokens, width), BF),
        pltpu.VMEM((SIDE, tokens, feats), BF),
        pltpu.VMEM((2, halftok, feats), BF),
        pltpu.VMEM((2, tokens, feats), BF),
        pltpu.VMEM((hidden, rows), BF),
        pltpu.VMEM((rows, every), F32),
        pltpu.VMEM((tokens, feats), BF),
        pltpu.SemaphoreType.DMA((7,)),
        pltpu.SemaphoreType.DMA((3,)),
        pltpu.SemaphoreType.DMA((6,)),
        pltpu.SemaphoreType.DMA((count,)),
    ]
    return kernel, scratch


def finish_of(rows, hidden):
    size, base = shares(hidden)
    n = 3 * size[1] // 2
    cut = n - size[1]

    def finish(dx_in, sum_in, late_in, dx_out, gate_out, up_out, down_out,
               DX, SUM, LATE, UP, GATE, DOWN, ins, outs):
        first = slice(0, base[1])
        last = slice(base[1], base[1] + 3 * size[1])
        loads = [
            pltpu.make_async_copy(sum_in.at[:, first], SUM.at[:, first], ins.at[0]),
            pltpu.make_async_copy(sum_in.at[:, last], SUM.at[:, last], ins.at[1]),
            pltpu.make_async_copy(late_in, LATE, ins.at[2]),
            pltpu.make_async_copy(dx_in, DX, ins.at[3]),
        ]
        for load in loads:
            load.start()
        h = size[0]
        loads[0].wait()
        DOWN[0:h, :] = SUM[:, 2 * h : 3 * h].T
        GATE[:, 0:h] = SUM[:, 0:h]
        UP[:, 0:h] = SUM[:, h : 2 * h]
        for load in loads[1:]:
            load.wait()
        at = base[1]
        total = [SUM[:, at + k * n : at + (k + 1) * n] + LATE[k, 0].astype(F32) + LATE[k, 1].astype(F32)
                 for k in (0, 1)]
        DOWN[h:hidden, :] = total[1][:, cut:n].T
        GATE[:, h:hidden] = total[0][:, 0 : size[1]]
        UP[:, h : h + cut] = total[0][:, size[1] : n]
        UP[:, h + cut : hidden] = total[1][:, 0:cut]
        stores = [
            pltpu.make_async_copy(DX, dx_out, outs.at[0]),
            pltpu.make_async_copy(GATE, gate_out, outs.at[1]),
            pltpu.make_async_copy(UP, up_out, outs.at[2]),
            pltpu.make_async_copy(DOWN, down_out, outs.at[3]),
        ]
        for copy in stores:
            copy.start()
        for copy in stores:
            copy.wait()

    return finish


def solution(mesh):
    def on_device(layer_input, out_cotangent, gate_matrix, up_matrix, down_matrix):
        tokens, feats = layer_input.shape
        rows, hidden = gate_matrix.shape
        width = feats * mesh.shape["tp"]
        kernel, scratch = kernel_of(rows, tokens, width, hidden)
        flops = 2 * 8 * tokens * width * hidden
        late = (2, 2, rows, shares(hidden)[0][1] * 3 // 2)
        any_space = pl.BlockSpec(memory_space=pl.ANY)
        dx, sums, lates = pl.pallas_call(
            kernel,
            out_shape=(
                jax.ShapeDtypeStruct((tokens, feats), BF),
                jax.ShapeDtypeStruct((rows, 3 * hidden), F32),
                jax.ShapeDtypeStruct(late, BF),
            ),
            in_specs=[any_space] * 5,
            out_specs=[any_space] * 3,
            scratch_shapes=scratch,
            compiler_params=pltpu.CompilerParams(
                collective_id=0, has_side_effects=True, vmem_limit_bytes=66_000_000),
            cost_estimate=pl.CostEstimate(
                flops=flops, bytes_accessed=4 << 20, transcendentals=tokens * hidden),
        )(layer_input, out_cotangent, gate_matrix, up_matrix, down_matrix)
        return pl.pallas_call(
            finish_of(rows, hidden),
            out_shape=(
                jax.ShapeDtypeStruct((tokens, feats), BF),
                jax.ShapeDtypeStruct((rows, hidden), F32),
                jax.ShapeDtypeStruct((rows, hidden), F32),
                jax.ShapeDtypeStruct((hidden, rows), F32),
            ),
            in_specs=[any_space] * 3,
            out_specs=[any_space] * 4,
            scratch_shapes=[
                pltpu.VMEM((tokens, feats), BF),
                pltpu.VMEM((rows, 3 * hidden), F32),
                pltpu.VMEM(late, BF),
                pltpu.VMEM((rows, hidden), F32),
                pltpu.VMEM((rows, hidden), F32),
                pltpu.VMEM((hidden, rows), F32),
                pltpu.SemaphoreType.DMA((4,)),
                pltpu.SemaphoreType.DMA((4,)),
            ],
        )(dx, sums, lates)

    return jax.shard_map(
        on_device, mesh=mesh,
        in_specs=(P("fs", "tp"), P("fs", "tp"), P("fs", "tp"), P("fs", "tp"), P("tp", "fs")),
        out_specs=(P("fs", "tp"), P("fs", "tp"), P("fs", "tp"), P("tp", "fs")),
        check_vma=False)
```

```python
import jax
import jax.numpy as jnp
from jax import lax
from jax.experimental import pallas as pl
from jax.experimental.pallas import tpu as pltpu
from jax.sharding import PartitionSpec as P

MESH = pl.DeviceIdType.MESH
BF = jnp.bfloat16
F32 = jnp.float32
SIDE = 4
ORDER = (2, 1, -1, 0)


def shares(hidden):
    first = 2 * hidden // 3
    return (first, hidden - first), (0, 3 * first)


def kernel_of(rows, tokens, width, hidden):
    size, base = shares(hidden)
    half = rows // 2
    feats = width // 8
    band = SIDE * rows
    halftok = tokens // 2
    every = 3 * hidden

    def kernel(x_in, q_in, gate_in, up_in, down_in, dx_out, sum_out, late_out,
               W, XQ, ACC, D, G, R1a, R1b, R2a, R2b, R3a, R3b, R4a, PD, E0, E1, E2, DN, SUM, DX,
               load_sem, store_sem, ss, rs):
        R1, R2, R3, R4 = (R1a, R1b), (R2a, R2b), (R3a, R3b), (R4a, late_out)
        fs, tp = lax.axis_index("fs"), lax.axis_index("tp")
        z, y = fs // SIDE, fs % SIDE
        x, c = tp // 2, tp % 2

        def turn(a, o):
            return (a + (o % SIDE)) % SIDE

        def fs_dev(f):
            return {"fs": f, "tp": tp}

        def tp_dev(t):
            return {"fs": fs, "tp": t}

        def big_dev(k, d):
            return fs_dev(turn(z, d) * SIDE + y) if k == 0 else fs_dev(z * SIDE + turn(y, d))

        def small_dev(k, d):
            return big_dev(1 - k, d)

        sibling = tp_dev(x * 2 + (1 - c))

        def x_dev(d):
            return tp_dev(turn(x, d) * 2 + c)

        barrier = pltpu.get_barrier_semaphore()
        for partner in (big_dev(0, 1), big_dev(0, -1), big_dev(1, 1), big_dev(1, -1),
                        x_dev(1), x_dev(-1), sibling):
            pl.semaphore_signal(barrier, inc=1, device_id=partner, device_id_type=MESH)
        mine = pl.ds(pl.multiple_of(fs * rows, rows), rows)
        my_feats = pl.ds(pl.multiple_of(tp * feats, feats), feats)
        loads = []

        def load(src, dst):
            copy = pltpu.make_async_copy(src, dst, load_sem.at[len(loads)])
            copy.start()
            loads.append(copy)

        for p in (0, 1):
            at, h, from_ = base[p], size[p], p * size[0]
            for i, ref in enumerate((gate_in, up_in)):
                load(ref.at[:, from_ : from_ + h], W.at[mine, at + i * h : at + (i + 1) * h])
            if p == 0:
                load(down_in, DN)
                load(x_in, XQ.at[0:tokens, my_feats])
                load(q_in, XQ.at[tokens : 2 * tokens, my_feats])

        def turn_down():
            loads[2].wait()
            turned = DN[...].astype(F32).T.astype(BF)
            for p in (0, 1):
                at, h, from_ = base[p], size[p], p * size[0]
                W[mine, at + 2 * h : at + 3 * h] = turned[:, from_ : from_ + h]

        def meet():
            pl.semaphore_wait(barrier, 7)

        meet()

        slots = {}

        def slot(name):
            if name not in slots:
                slots[name] = len(slots)
            return slots[name]

        def send(group, name, src, dst, dev):
            pltpu.make_async_remote_copy(
                src_ref=src, dst_ref=dst, send_sem=ss.at[group], recv_sem=rs.at[slot(name)],
                device_id=dev, device_id_type=MESH).start()

        def awaited(name, like):
            return pltpu.make_async_remote_copy(
                src_ref=like, dst_ref=like, send_sem=ss.at[0], recv_sem=rs.at[slot(name)],
                device_id=sibling, device_id_type=MESH)

        def arrived(name, like):
            awaited(name, like).wait_recv()

        def left(group, like):
            pltpu.make_async_remote_copy(
                src_ref=like, dst_ref=like, send_sem=ss.at[group], recv_sem=rs.at[0],
                device_id=sibling, device_id_type=MESH).wait_send()

        def block(k, so, bo, part=None):
            zo, yo = (bo, so) if k == 0 else (so, bo)
            start = (turn(z, zo) * SIDE + turn(y, yo)) * rows
            if part is None:
                return pl.ds(pl.multiple_of(start, rows), rows)
            return pl.ds(pl.multiple_of(start + part * half, half), half)

        def lanes(p, k):
            cols = 3 * size[p] // 2
            return slice(base[p] + k * cols, base[p] + (k + 1) * cols)

        def blocks(ref, p, n):
            return ref.at[0 : n * rows, base[p] : base[p] + 3 * size[p]]

        def w(p, k, so, bo, part=None):
            return W.at[block(k, so, bo, part), lanes(p, k)]

        def near(p, k):
            for d in (1, -1):
                send(p, ("a1", p), w(p, k, 0, 0), w(p, k, 0, 0), small_dev(k, d))

        def far(p, r):
            for k in (0, 1):
                for d in (1, -1):
                    send(p, ("a3", p, r), w(p, k, r, 0), w(p, k, r, 0), big_dev(k, d))

        def near_arrived(p):
            arrived(("a1", p), blocks(W, p, 2))
            for k in (0, 1):
                for i, d in enumerate((1, -1)):
                    send(p, ("a2", p), w(p, k, -d, 0, i), w(p, k, -d, 0, i), small_dev(k, d))

        def opposite_arrived(p):
            arrived(("a2", p), blocks(W, p, 1))

        def far_arrived(p, r):
            arrived(("a3", p, r), blocks(W, p, 2))
            for k in (0, 1):
                for i, d in enumerate((1, -1)):
                    send(p, ("a4", p), w(p, k, r, -d, i), w(p, k, r, -d, i), big_dev(k, d))

        def last_arrived(p):
            arrived(("a4", p), blocks(W, p, 4))

        def xq(xo, core, part):
            start = (turn(x, xo) * 2 + core) * feats
            lane = pl.ds(pl.multiple_of(start, feats), feats)
            return XQ.at[part * tokens : (part + 1) * tokens, lane]

        def x_own(i):
            for d in (1, -1):
                part = i if d == 1 else 1 - i
                send(2, ("x1", i), xq(0, c, part), xq(0, c, part), x_dev(d))

        def to_sibling(xo, part):
            send(2, "sib", xq(xo, c, part), xq(xo, c, part), sibling)

        def x_first():
            arrived(("x1", 0), XQ.at[:, 0:feats])
            for i, d in enumerate((1, -1)):
                send(2, "x2", xq(-d, c, i), xq(-d, c, i), x_dev(d))
            for i, d in enumerate((1, -1)):
                to_sibling(-d, i)

        def x_second():
            arrived(("x1", 1), XQ.at[:, 0:feats])
            for i, d in enumerate((1, -1)):
                to_sibling(-d, 1 - i)

        def x_third():
            arrived("x2", XQ.at[:, 0:feats])
            for i in (0, 1):
                to_sibling(2, i)

        def x_last():
            arrived("sib", XQ.at[:, 0 : 4 * feats])

        loads[0].wait()
        loads[1].wait()
        near(0, 0)
        turn_down()
        near(0, 1)
        far(0, 0)
        loads[3].wait()
        loads[4].wait()
        x_own(0)
        x_own(1)
        for part in (0, 1):
            to_sibling(0, part)
        loads[5].wait()
        loads[6].wait()
        for k in (0, 1):
            near(1, k)

        near_arrived(0)
        for r in (1, -1):
            far(0, r)
        x_first()
        far_arrived(0, 0)
        near_arrived(1)
        opposite_arrived(0)
        far(0, 2)
        far_arrived(0, 1)
        x_second()
        far_arrived(0, -1)
        far(1, 0)
        x_third()
        far_arrived(0, 2)
        for r in (1, -1):
            far(1, r)
        opposite_arrived(1)
        far(1, 2)
        x_last()

        tile = tokens // 3

        def dot(a, b, dims):
            return lax.dot_general(a, b, (dims, ((), ())), preferred_element_type=F32)

        def put(at, lane, value, first):
            if first:
                ACC[at, lane] = value
            else:
                ACC[at, lane] += value

        def forward(p, k, o, first=False):
            both = lanes(p, k)
            split = base[p] + 2 * size[p]

            def piece(m, carry):
                at = pl.ds(pl.multiple_of(m * tile, tile), tile)
                low = pl.ds(pl.multiple_of(tokens + m * tile, tile), tile)
                if k == 0:
                    span = pl.ds(pl.multiple_of(turn(z, o) * band, band), band)
                    put(at, both, dot(XQ[at, span], W[span, both], ((1,), (0,))), first)
                else:
                    spans = [pl.ds(pl.multiple_of(i * band + turn(y, o) * rows, rows), rows)
                             for i in range(SIDE)]
                    for top, lane in ((at, slice(both.start, split)), (low, slice(split, both.stop))):
                        a = jnp.concatenate([XQ[top, s] for s in spans], axis=1)
                        b = jnp.concatenate([W[s, lane] for s in spans], axis=0)
                        put(at, lane, dot(a, b, ((1,), (0,))), first)
                return carry
            lax.fori_loop(0, 3, piece, 0)

        step = tokens // 24

        def gate(p):
            h = size[p]
            one, two, three, four = (base[p] + i * h for i in range(4))

            def piece(m, carry):
                at = pl.ds(pl.multiple_of(m * step, step), step)
                g = ACC[at, one:two]
                u = ACC[at, two:three]
                e = ACC[at, three:four]
                s = jax.nn.sigmoid(g)
                act = g * s
                D[at, one:two] = (e * u * s * (1.0 + g * (1.0 - s))).astype(BF)
                D[at, two:three] = (e * act).astype(BF)
                D[at, three:four] = (act * u).astype(BF)
                return carry

            lax.fori_loop(0, 24, piece, 0)

        def grads(p, k, o):
            both = lanes(p, k)
            split = base[p] + 2 * size[p]

            def piece(n, carry):
                if k == 0:
                    span = pl.ds(pl.multiple_of(turn(z, o) * band + n * 2 * rows, 2 * rows), 2 * rows)
                    G[span, both] = dot(XQ[0:tokens, span], D[:, both], ((0,), (0,))).astype(BF)
                else:
                    spans = [pl.ds(pl.multiple_of((2 * n + i) * band + turn(y, o) * rows, rows), rows)
                             for i in range(2)]
                    for top, lane in ((0, slice(both.start, split)), (tokens, slice(split, both.stop))):
                        a = jnp.concatenate([XQ[top : top + tokens, s] for s in spans], axis=1)
                        r = dot(a, D[:, lane], ((0,), (0,))).astype(BF)
                        for i in range(2):
                            G[spans[i], lane] = r[i * rows : (i + 1) * rows]
                return carry
            lax.fori_loop(0, 2, piece, 0)

        def g(p, k, so, bo, part=None):
            return G.at[block(k, so, bo, part), lanes(p, k)]

        def add_into(ref, *others):
            def piece(m, carry):
                at = pl.ds(pl.multiple_of(m * 16, 16), 16)
                total = ref[at, :].astype(F32)
                for other in others:
                    total = total + other[at, :].astype(F32)
                ref[at, :] = total.astype(BF)
                return carry
            lax.fori_loop(0, ref.shape[0] // 16, piece, 0)

        def s1(p):
            for j, r in enumerate(ORDER):
                for k in (0, 1):
                    for i, d in enumerate((1, -1)):
                        send(3 + p, ("g1", p, j), g(p, k, r, 2, i), R1[p].at[k, i, j],
                             big_dev(k, d))

        def s2(p, j):
            r = ORDER[j]
            arrived(("g1", p, j), blocks(G, p, 1))
            for k in (0, 1):
                for i, d in enumerate((1, -1)):
                    add_into(g(p, k, r, d, i), R1[p].at[k, i, j])
            for k in (0, 1):
                for i, d in enumerate((1, -1)):
                    send(3 + p, ("g2", p, j), g(p, k, r, d), R2[p].at[k, i, j], big_dev(k, d))

        def two(p, j):
            arrived(("g2", p, j), blocks(G, p, 2))

        def s3(p):
            two(p, 0)
            for k in (0, 1):
                add_into(g(p, k, 2, 0), R2[p].at[k, 0, 0], R2[p].at[k, 1, 0])
            for k in (0, 1):
                for i, d in enumerate((1, -1)):
                    send(3 + p, ("g3", p), g(p, k, 2, 0, i), R3[p].at[k, i], small_dev(k, d))

        def pre4(p):
            for i, d in enumerate((1, -1)):
                two(p, 1 + i)
                for k in (0, 1):
                    add_into(g(p, k, d, 0), R2[p].at[k, 0, 1 + i], R2[p].at[k, 1, 1 + i])

        def s4(p):
            arrived(("g3", p), blocks(G, p, 1))
            for k in (0, 1):
                for i, d in enumerate((1, -1)):
                    add_into(g(p, k, d, 0, i), R3[p].at[k, i])
            for k in (0, 1):
                for i, d in enumerate((1, -1)):
                    send(3 + p, ("g4", p), g(p, k, d, 0), R4[p].at[k, i], small_dev(k, d))

        def keep(p, k, *others):
            own, to = g(p, k, 0, 0), SUM.at[:, lanes(p, k)]

            def piece(m, carry):
                at = pl.ds(pl.multiple_of(m * 16, 16), 16)
                total = own[at, :].astype(F32)
                for other in others:
                    total = total + other[at, :].astype(F32)
                to[at, :] = total
                return carry

            lax.fori_loop(0, rows // 16, piece, 0)

        def partial_of(xo, core):
            start = (turn(x, xo) * 2 + core) * feats
            span = pl.ds(pl.multiple_of(start, feats), feats)

            def piece(m, carry):
                at = pl.ds(pl.multiple_of(m * tile, tile), tile)
                total = 0.0
                for p in (0, 1):
                    lane = slice(base[p], base[p] + 2 * size[p])
                    total = total + dot(D[at, lane], W[span, lane], ((1,), (1,)))
                PD[at, span] = total.astype(BF)
                return carry
            lax.fori_loop(0, 3, piece, 0)

        def pd(xo, core, part=None):
            start = (turn(x, xo) * 2 + core) * feats
            lane = pl.ds(pl.multiple_of(start, feats), feats)
            if part is None:
                return PD.at[:, lane]
            return PD.at[part * halftok : (part + 1) * halftok, lane]

        for o in (0, 1, -1):
            for k in (0, 1):
                forward(0, k, o, o == 0)
        far_arrived(1, 0)
        last_arrived(0)
        for k in (0, 1):
            forward(0, k, 2)
        gate(0)
        far_arrived(1, 1)
        far_arrived(1, -1)
        for k in (0, 1):
            grads(0, k, 2)
        far_arrived(1, 2)
        s1(0)
        for o in (1, -1):
            for k in (0, 1):
                grads(0, k, o)

        for j, o in enumerate((0, 1, -1)):
            for k in (0, 1):
                forward(1, k, o, o == 0)
            s2(0, j)
        last_arrived(1)
        for k in (0, 1):
            forward(1, k, 2)
        gate(1)
        for k in (0, 1):
            grads(1, k, 2)
        s1(1)
        for o in (1, -1):
            for k in (0, 1):
                grads(1, k, o)
        for k in (0, 1):
            grads(0, k, 0)
        s3(0)
        s2(0, 3)
        for j, r in enumerate(ORDER):
            partial_of(r, 1 - c)
            send(5, ("d0", j), pd(r, 1 - c), E0.at[j], sibling)

        def sibling_sum(j):
            arrived(("d0", j), PD.at[:, 0:feats])
            add_into(pd(ORDER[j], c), E0.at[j])

        partial_of(2, c)
        sibling_sum(0)
        for i, d in enumerate((1, -1)):
            send(5, "d1", pd(2, c, i), E1.at[i], x_dev(d))
        for j in (1, 2):
            partial_of(ORDER[j], c)
            sibling_sum(j)
        for j in (0, 1, 2):
            s2(1, j)
        pre4(0)
        partial_of(0, c)
        s4(0)
        arrived("d1", PD.at[:, 0:feats])
        for i, d in enumerate((1, -1)):
            add_into(pd(d, c, i), E1.at[i])
            send(5, "d2", pd(d, c), E2.at[i], x_dev(d))
        for k in (0, 1):
            grads(1, k, 0)
        s3(1)
        s2(1, 3)
        pre4(1)

        stores = []

        def store(src, dst):
            copy = pltpu.make_async_copy(src, dst, store_sem.at[len(stores)])
            copy.start()
            stores.append(copy)

        def finish_dx():
            arrived(("d0", 3), PD.at[:, 0:feats])
            arrived("d2", PD.at[:, 0 : 2 * feats])
            own = pd(0, c)

            def piece(m, carry):
                at = pl.ds(pl.multiple_of(m * 16, 16), 16)
                total = (own[at, :].astype(F32) + E0[3, at, :].astype(F32)
                         + E2[0, at, :].astype(F32) + E2[1, at, :].astype(F32))
                DX[at, :] = total.astype(BF)
                return carry

            lax.fori_loop(0, tokens // 16, piece, 0)
            store(DX, dx_out)

        def finish_grads(p):
            two(p, 3)
            if p == 0:
                arrived(("g4", p), blocks(G, p, 2))
            for k in (0, 1):
                late = [R4[p].at[k, i] for i in (0, 1)] if p == 0 else []
                keep(p, k, R2[p].at[k, 0, 3], R2[p].at[k, 1, 3], *late)
            at = slice(base[p], base[p] + 3 * size[p])
            store(SUM.at[:, at], sum_out.at[:, at])

        finish_dx()
        s4(1)
        finish_grads(0)
        finish_grads(1)
        for p in (0, 1):
            left(p, blocks(W, p, 15))
            left(3 + p, blocks(G, p, 15))
        left(2, XQ.at[:, 0 : 7 * feats])
        left(5, PD.at[:, 0 : 7 * feats])
        for copy in stores:
            copy.wait()
        arrived(("g4", 1), blocks(G, 1, 2))

    count = 2 * (1 + 1 + 4 + 1) + 4 + 2 * (4 + 4 + 1 + 1) + 4 + 1 + 1
    n = [3 * h // 2 for h in size]
    scratch = [
        pltpu.VMEM((width, every), BF),
        pltpu.VMEM((2 * tokens, width), BF),
        pltpu.VMEM((tokens, every), F32),
        pltpu.VMEM((tokens, every), BF),
        pltpu.VMEM((width, every), BF),
        *[pltpu.VMEM((2, 2, SIDE, half, m), BF) for m in n],
        *[pltpu.VMEM((2, 2, SIDE, rows, m), BF) for m in n],
        *[pltpu.VMEM((2, 2, half, m), BF) for m in n],
        pltpu.VMEM((2, 2, rows, n[0]), BF),
        pltpu.VMEM((tokens, width), BF),
        pltpu.VMEM((SIDE, tokens, feats), BF),
        pltpu.VMEM((2, halftok, feats), BF),
        pltpu.VMEM((2, tokens, feats), BF),
        pltpu.VMEM((hidden, rows), BF),
        pltpu.VMEM((rows, every), F32),
        pltpu.VMEM((tokens, feats), BF),
        pltpu.SemaphoreType.DMA((7,)),
        pltpu.SemaphoreType.DMA((3,)),
        pltpu.SemaphoreType.DMA((6,)),
        pltpu.SemaphoreType.DMA((count,)),
    ]
    return kernel, scratch


def finish_of(rows, hidden):
    size, base = shares(hidden)
    n = 3 * size[1] // 2
    cut = n - size[1]

    def finish(dx_in, sum_in, late_in, dx_out, gate_out, up_out, down_out,
               DX, SUM, LATE, UP, GATE, DOWN, ins, outs):
        first = slice(0, base[1])
        last = slice(base[1], base[1] + 3 * size[1])
        loads = [
            pltpu.make_async_copy(sum_in.at[:, first], SUM.at[:, first], ins.at[0]),
            pltpu.make_async_copy(sum_in.at[:, last], SUM.at[:, last], ins.at[1]),
            pltpu.make_async_copy(late_in, LATE, ins.at[2]),
            pltpu.make_async_copy(dx_in, DX, ins.at[3]),
        ]
        for load in loads:
            load.start()
        h, at = size[0], base[1]
        stores = []

        def store(src, dst):
            copy = pltpu.make_async_copy(src, dst, outs.at[len(stores)])
            copy.start()
            stores.append(copy)

        loads[0].wait()
        store(SUM.at[:, 0:h], gate_out.at[:, 0:h])
        store(SUM.at[:, h : 2 * h], up_out.at[:, 0:h])
        DOWN[0:h, :] = SUM[:, 2 * h : 3 * h].T
        store(DOWN.at[0:h, :], down_out.at[0:h, :])
        loads[1].wait()
        loads[2].wait()
        total = [SUM[:, at + k * n : at + (k + 1) * n] + LATE[k, 0].astype(F32) + LATE[k, 1].astype(F32)
                 for k in (0, 1)]
        GATE[...] = total[0][:, 0 : size[1]]
        store(GATE, gate_out.at[:, h:hidden])
        UP[:, 0:cut] = total[0][:, size[1] : n]
        UP[:, cut : size[1]] = total[1][:, 0:cut]
        store(UP, up_out.at[:, h:hidden])
        DOWN[h:hidden, :] = total[1][:, cut:n].T
        store(DOWN.at[h:hidden, :], down_out.at[h:hidden, :])
        loads[3].wait()
        store(DX, dx_out)
        for copy in stores:
            copy.wait()

    return finish


def solution(mesh):
    def on_device(layer_input, out_cotangent, gate_matrix, up_matrix, down_matrix):
        tokens, feats = layer_input.shape
        rows, hidden = gate_matrix.shape
        width = feats * mesh.shape["tp"]
        kernel, scratch = kernel_of(rows, tokens, width, hidden)
        flops = 2 * 8 * tokens * width * hidden
        late = (2, 2, rows, shares(hidden)[0][1] * 3 // 2)
        any_space = pl.BlockSpec(memory_space=pl.ANY)
        dx, sums, lates = pl.pallas_call(
            kernel,
            out_shape=(
                jax.ShapeDtypeStruct((tokens, feats), BF),
                jax.ShapeDtypeStruct((rows, 3 * hidden), F32),
                jax.ShapeDtypeStruct(late, BF),
            ),
            in_specs=[any_space] * 5,
            out_specs=[any_space] * 3,
            scratch_shapes=scratch,
            compiler_params=pltpu.CompilerParams(
                collective_id=0, has_side_effects=True, vmem_limit_bytes=66_000_000),
            cost_estimate=pl.CostEstimate(
                flops=flops, bytes_accessed=4 << 20, transcendentals=tokens * hidden),
        )(layer_input, out_cotangent, gate_matrix, up_matrix, down_matrix)
        return pl.pallas_call(
            finish_of(rows, hidden),
            out_shape=(
                jax.ShapeDtypeStruct((tokens, feats), BF),
                jax.ShapeDtypeStruct((rows, hidden), F32),
                jax.ShapeDtypeStruct((rows, hidden), F32),
                jax.ShapeDtypeStruct((hidden, rows), F32),
            ),
            in_specs=[any_space] * 3,
            out_specs=[any_space] * 4,
            scratch_shapes=[
                pltpu.VMEM((tokens, feats), BF),
                pltpu.VMEM((rows, 3 * hidden), F32),
                pltpu.VMEM(late, BF),
                pltpu.VMEM((rows, shares(hidden)[0][1]), F32),
                pltpu.VMEM((rows, shares(hidden)[0][1]), F32),
                pltpu.VMEM((hidden, rows), F32),
                pltpu.SemaphoreType.DMA((4,)),
                pltpu.SemaphoreType.DMA((7,)),
            ],
        )(dx, sums, lates)

    return jax.shard_map(
        on_device, mesh=mesh,
        in_specs=(P("fs", "tp"), P("fs", "tp"), P("fs", "tp"), P("fs", "tp"), P("tp", "fs")),
        out_specs=(P("fs", "tp"), P("fs", "tp"), P("fs", "tp"), P("tp", "fs")),
        check_vma=False)
```

```python
import jax
import jax.numpy as jnp
from jax import lax
from jax.experimental import pallas as pl
from jax.experimental.pallas import tpu as pltpu
from jax.sharding import PartitionSpec as P

MESH = pl.DeviceIdType.MESH
BF = jnp.bfloat16
F32 = jnp.float32
SIDE = 4
ORDER = (2, 1, -1, 0)


def shares(hidden):
    first = 2 * hidden // 3
    return (first, hidden - first), (0, 3 * first)


def kernel_of(rows, tokens, width, hidden):
    size, base = shares(hidden)
    half = rows // 2
    feats = width // 8
    band = SIDE * rows
    halftok = tokens // 2
    every = 3 * hidden

    def kernel(x_in, q_in, gate_in, up_in, down_in, dx_out, sum_out, late_out,
               W, XQ, ACC, D, G, R1a, R1b, R2a, R2b, R3a, R3b, R4a, PD, E0, E1, E2, DN, SUM, DX,
               load_sem, store_sem, ss, rs):
        R1, R2, R3, R4 = (R1a, R1b), (R2a, R2b), (R3a, R3b), (R4a, late_out)
        fs, tp = lax.axis_index("fs"), lax.axis_index("tp")
        z, y = fs // SIDE, fs % SIDE
        x, c = tp // 2, tp % 2

        def turn(a, o):
            return (a + (o % SIDE)) % SIDE

        def fs_dev(f):
            return {"fs": f, "tp": tp}

        def tp_dev(t):
            return {"fs": fs, "tp": t}

        def big_dev(k, d):
            return fs_dev(turn(z, d) * SIDE + y) if k == 0 else fs_dev(z * SIDE + turn(y, d))

        def small_dev(k, d):
            return big_dev(1 - k, d)

        sibling = tp_dev(x * 2 + (1 - c))

        def x_dev(d):
            return tp_dev(turn(x, d) * 2 + c)

        barrier = pltpu.get_barrier_semaphore()
        for partner in (big_dev(0, 1), big_dev(0, -1), big_dev(1, 1), big_dev(1, -1),
                        x_dev(1), x_dev(-1), sibling):
            pl.semaphore_signal(barrier, inc=1, device_id=partner, device_id_type=MESH)
        mine = pl.ds(pl.multiple_of(fs * rows, rows), rows)
        my_feats = pl.ds(pl.multiple_of(tp * feats, feats), feats)
        loads = []

        def load(src, dst):
            copy = pltpu.make_async_copy(src, dst, load_sem.at[len(loads)])
            copy.start()
            loads.append(copy)

        for p in (0, 1):
            at, h, from_ = base[p], size[p], p * size[0]
            for i, ref in enumerate((gate_in, up_in)):
                load(ref.at[:, from_ : from_ + h], W.at[mine, at + i * h : at + (i + 1) * h])
            if p == 0:
                load(down_in, DN)
                load(x_in, XQ.at[0:tokens, my_feats])
                load(q_in, XQ.at[tokens : 2 * tokens, my_feats])

        def turn_down():
            loads[2].wait()
            turned = DN[...].astype(F32).T.astype(BF)
            for p in (0, 1):
                at, h, from_ = base[p], size[p], p * size[0]
                W[mine, at + 2 * h : at + 3 * h] = turned[:, from_ : from_ + h]

        def meet():
            pl.semaphore_wait(barrier, 7)

        meet()

        slots = {}

        def slot(name):
            if name not in slots:
                slots[name] = len(slots)
            return slots[name]

        def send(group, name, src, dst, dev):
            pltpu.make_async_remote_copy(
                src_ref=src, dst_ref=dst, send_sem=ss.at[group], recv_sem=rs.at[slot(name)],
                device_id=dev, device_id_type=MESH).start()

        def awaited(name, like):
            return pltpu.make_async_remote_copy(
                src_ref=like, dst_ref=like, send_sem=ss.at[0], recv_sem=rs.at[slot(name)],
                device_id=sibling, device_id_type=MESH)

        def arrived(name, like):
            awaited(name, like).wait_recv()

        def left(group, like):
            pltpu.make_async_remote_copy(
                src_ref=like, dst_ref=like, send_sem=ss.at[group], recv_sem=rs.at[0],
                device_id=sibling, device_id_type=MESH).wait_send()

        def block(k, so, bo, part=None):
            zo, yo = (bo, so) if k == 0 else (so, bo)
            start = (turn(z, zo) * SIDE + turn(y, yo)) * rows
            if part is None:
                return pl.ds(pl.multiple_of(start, rows), rows)
            return pl.ds(pl.multiple_of(start + part * half, half), half)

        def lanes(p, k):
            cols = 3 * size[p] // 2
            return slice(base[p] + k * cols, base[p] + (k + 1) * cols)

        def blocks(ref, p, n):
            return ref.at[0 : n * rows, base[p] : base[p] + 3 * size[p]]

        def w(p, k, so, bo, part=None):
            return W.at[block(k, so, bo, part), lanes(p, k)]

        def near(p, k):
            for d in (1, -1):
                send(p, ("a1", p), w(p, k, 0, 0), w(p, k, 0, 0), small_dev(k, d))

        def far(p, r):
            for k in (0, 1):
                for d in (1, -1):
                    send(p, ("a3", p, r), w(p, k, r, 0), w(p, k, r, 0), big_dev(k, d))

        def near_arrived(p):
            arrived(("a1", p), blocks(W, p, 2))
            for k in (0, 1):
                for i, d in enumerate((1, -1)):
                    send(p, ("a2", p), w(p, k, -d, 0, i), w(p, k, -d, 0, i), small_dev(k, d))

        def opposite_arrived(p):
            arrived(("a2", p), blocks(W, p, 1))

        def far_arrived(p, r):
            arrived(("a3", p, r), blocks(W, p, 2))
            for k in (0, 1):
                for i, d in enumerate((1, -1)):
                    send(p, ("a4", p), w(p, k, r, -d, i), w(p, k, r, -d, i), big_dev(k, d))

        def last_arrived(p):
            arrived(("a4", p), blocks(W, p, 4))

        def xq(xo, core, part):
            start = (turn(x, xo) * 2 + core) * feats
            lane = pl.ds(pl.multiple_of(start, feats), feats)
            return XQ.at[part * tokens : (part + 1) * tokens, lane]

        def x_own(i):
            for d in (1, -1):
                part = i if d == 1 else 1 - i
                send(2, ("x1", i), xq(0, c, part), xq(0, c, part), x_dev(d))

        def to_sibling(xo, part):
            send(2, "sib", xq(xo, c, part), xq(xo, c, part), sibling)

        def x_first():
            arrived(("x1", 0), XQ.at[:, 0:feats])
            for i, d in enumerate((1, -1)):
                send(2, "x2", xq(-d, c, i), xq(-d, c, i), x_dev(d))
            for i, d in enumerate((1, -1)):
                to_sibling(-d, i)

        def x_second():
            arrived(("x1", 1), XQ.at[:, 0:feats])
            for i, d in enumerate((1, -1)):
                to_sibling(-d, 1 - i)

        def x_third():
            arrived("x2", XQ.at[:, 0:feats])
            for i in (0, 1):
                to_sibling(2, i)

        def x_last():
            arrived("sib", XQ.at[:, 0 : 4 * feats])

        loads[0].wait()
        loads[1].wait()
        near(0, 0)
        turn_down()
        near(0, 1)
        far(0, 0)
        loads[3].wait()
        loads[4].wait()
        x_own(0)
        x_own(1)
        for part in (0, 1):
            to_sibling(0, part)
        loads[5].wait()
        loads[6].wait()
        for k in (0, 1):
            near(1, k)

        near_arrived(0)
        for r in (1, -1):
            far(0, r)
        x_first()
        far_arrived(0, 0)
        near_arrived(1)
        opposite_arrived(0)
        far(0, 2)
        far_arrived(0, 1)
        x_second()
        far_arrived(0, -1)
        far(1, 0)
        x_third()
        far_arrived(0, 2)
        for r in (1, -1):
            far(1, r)
        opposite_arrived(1)
        far(1, 2)
        x_last()

        tile = tokens // 3

        def dot(a, b, dims):
            return lax.dot_general(a, b, (dims, ((), ())), preferred_element_type=F32)

        def put(at, lane, value, first):
            if first:
                ACC[at, lane] = value
            else:
                ACC[at, lane] += value

        def forward(p, k, o, first=False):
            both = lanes(p, k)
            split = base[p] + 2 * size[p]

            def piece(m, carry):
                at = pl.ds(pl.multiple_of(m * tile, tile), tile)
                low = pl.ds(pl.multiple_of(tokens + m * tile, tile), tile)
                if k == 0:
                    span = pl.ds(pl.multiple_of(turn(z, o) * band, band), band)
                    put(at, both, dot(XQ[at, span], W[span, both], ((1,), (0,))), first)
                else:
                    spans = [pl.ds(pl.multiple_of(i * band + turn(y, o) * rows, rows), rows)
                             for i in range(SIDE)]
                    for top, lane in ((at, slice(both.start, split)), (low, slice(split, both.stop))):
                        a = jnp.concatenate([XQ[top, s] for s in spans], axis=1)
                        b = jnp.concatenate([W[s, lane] for s in spans], axis=0)
                        put(at, lane, dot(a, b, ((1,), (0,))), first)
                return carry
            lax.fori_loop(0, 3, piece, 0)

        step = tokens // 24

        def gate(p):
            h = size[p]
            one, two, three, four = (base[p] + i * h for i in range(4))

            def piece(m, carry):
                at = pl.ds(pl.multiple_of(m * step, step), step)
                g = ACC[at, one:two]
                u = ACC[at, two:three]
                e = ACC[at, three:four]
                s = 1.0 / (1.0 + jnp.exp(-g))
                act = g * s
                D[at, one:two] = (e * u * s * (1.0 + g * (1.0 - s))).astype(BF)
                D[at, two:three] = (e * act).astype(BF)
                D[at, three:four] = (act * u).astype(BF)
                return carry

            lax.fori_loop(0, 24, piece, 0)

        def grads(p, k, o):
            both = lanes(p, k)
            split = base[p] + 2 * size[p]

            def piece(n, carry):
                if k == 0:
                    span = pl.ds(pl.multiple_of(turn(z, o) * band + n * 2 * rows, 2 * rows), 2 * rows)
                    G[span, both] = dot(XQ[0:tokens, span], D[:, both], ((0,), (0,))).astype(BF)
                else:
                    spans = [pl.ds(pl.multiple_of((2 * n + i) * band + turn(y, o) * rows, rows), rows)
                             for i in range(2)]
                    for top, lane in ((0, slice(both.start, split)), (tokens, slice(split, both.stop))):
                        a = jnp.concatenate([XQ[top : top + tokens, s] for s in spans], axis=1)
                        r = dot(a, D[:, lane], ((0,), (0,))).astype(BF)
                        for i in range(2):
                            G[spans[i], lane] = r[i * rows : (i + 1) * rows]
                return carry
            lax.fori_loop(0, 2, piece, 0)

        def g(p, k, so, bo, part=None):
            return G.at[block(k, so, bo, part), lanes(p, k)]

        def add_into(ref, *others):
            def piece(m, carry):
                at = pl.ds(pl.multiple_of(m * 16, 16), 16)
                total = ref[at, :].astype(F32)
                for other in others:
                    total = total + other[at, :].astype(F32)
                ref[at, :] = total.astype(BF)
                return carry
            lax.fori_loop(0, ref.shape[0] // 16, piece, 0)

        def s1(p):
            for j, r in enumerate(ORDER):
                for k in (0, 1):
                    for i, d in enumerate((1, -1)):
                        send(3 + p, ("g1", p, j), g(p, k, r, 2, i), R1[p].at[k, i, j],
                             big_dev(k, d))

        def s2(p, j):
            r = ORDER[j]
            arrived(("g1", p, j), blocks(G, p, 1))
            for k in (0, 1):
                for i, d in enumerate((1, -1)):
                    add_into(g(p, k, r, d, i), R1[p].at[k, i, j])
            for k in (0, 1):
                for i, d in enumerate((1, -1)):
                    send(3 + p, ("g2", p, j), g(p, k, r, d), R2[p].at[k, i, j], big_dev(k, d))

        def two(p, j):
            arrived(("g2", p, j), blocks(G, p, 2))

        def s3(p):
            two(p, 0)
            for k in (0, 1):
                add_into(g(p, k, 2, 0), R2[p].at[k, 0, 0], R2[p].at[k, 1, 0])
            for k in (0, 1):
                for i, d in enumerate((1, -1)):
                    send(3 + p, ("g3", p), g(p, k, 2, 0, i), R3[p].at[k, i], small_dev(k, d))

        def pre4(p):
            for i, d in enumerate((1, -1)):
                two(p, 1 + i)
                for k in (0, 1):
                    add_into(g(p, k, d, 0), R2[p].at[k, 0, 1 + i], R2[p].at[k, 1, 1 + i])

        def s4(p):
            arrived(("g3", p), blocks(G, p, 1))
            for k in (0, 1):
                for i, d in enumerate((1, -1)):
                    add_into(g(p, k, d, 0, i), R3[p].at[k, i])
            for k in (0, 1):
                for i, d in enumerate((1, -1)):
                    send(3 + p, ("g4", p), g(p, k, d, 0), R4[p].at[k, i], small_dev(k, d))

        def keep(p, k, *others):
            own, to = g(p, k, 0, 0), SUM.at[:, lanes(p, k)]

            def piece(m, carry):
                at = pl.ds(pl.multiple_of(m * 16, 16), 16)
                total = own[at, :].astype(F32)
                for other in others:
                    total = total + other[at, :].astype(F32)
                to[at, :] = total
                return carry

            lax.fori_loop(0, rows // 16, piece, 0)

        def partial_of(xo, core):
            start = (turn(x, xo) * 2 + core) * feats
            span = pl.ds(pl.multiple_of(start, feats), feats)

            def piece(m, carry):
                at = pl.ds(pl.multiple_of(m * tile, tile), tile)
                total = 0.0
                for p in (0, 1):
                    lane = slice(base[p], base[p] + 2 * size[p])
                    total = total + dot(D[at, lane], W[span, lane], ((1,), (1,)))
                PD[at, span] = total.astype(BF)
                return carry
            lax.fori_loop(0, 3, piece, 0)

        def pd(xo, core, part=None):
            start = (turn(x, xo) * 2 + core) * feats
            lane = pl.ds(pl.multiple_of(start, feats), feats)
            if part is None:
                return PD.at[:, lane]
            return PD.at[part * halftok : (part + 1) * halftok, lane]

        for o in (0, 1, -1):
            for k in (0, 1):
                forward(0, k, o, o == 0)
        far_arrived(1, 0)
        last_arrived(0)
        for k in (0, 1):
            forward(0, k, 2)
        gate(0)
        far_arrived(1, 1)
        far_arrived(1, -1)
        for k in (0, 1):
            grads(0, k, 2)
        far_arrived(1, 2)
        s1(0)
        for o in (1, -1):
            for k in (0, 1):
                grads(0, k, o)

        for j, o in enumerate((0, 1, -1)):
            for k in (0, 1):
                forward(1, k, o, o == 0)
            s2(0, j)
        last_arrived(1)
        for k in (0, 1):
            forward(1, k, 2)
        gate(1)
        for k in (0, 1):
            grads(1, k, 2)
        s1(1)
        for o in (1, -1):
            for k in (0, 1):
                grads(1, k, o)
        for k in (0, 1):
            grads(0, k, 0)
        s3(0)
        s2(0, 3)
        for j, r in enumerate(ORDER):
            partial_of(r, 1 - c)
            send(5, ("d0", j), pd(r, 1 - c), E0.at[j], sibling)

        def sibling_sum(j):
            arrived(("d0", j), PD.at[:, 0:feats])
            add_into(pd(ORDER[j], c), E0.at[j])

        partial_of(2, c)
        sibling_sum(0)
        for i, d in enumerate((1, -1)):
            send(5, "d1", pd(2, c, i), E1.at[i], x_dev(d))
        for j in (1, 2):
            partial_of(ORDER[j], c)
            sibling_sum(j)
        for j in (0, 1, 2):
            s2(1, j)
        pre4(0)
        partial_of(0, c)
        s4(0)
        arrived("d1", PD.at[:, 0:feats])
        for i, d in enumerate((1, -1)):
            add_into(pd(d, c, i), E1.at[i])
            send(5, "d2", pd(d, c), E2.at[i], x_dev(d))
        for k in (0, 1):
            grads(1, k, 0)
        s3(1)
        s2(1, 3)
        pre4(1)

        stores = []

        def store(src, dst):
            copy = pltpu.make_async_copy(src, dst, store_sem.at[len(stores)])
            copy.start()
            stores.append(copy)

        def finish_dx():
            arrived(("d0", 3), PD.at[:, 0:feats])
            arrived("d2", PD.at[:, 0 : 2 * feats])
            own = pd(0, c)

            def piece(m, carry):
                at = pl.ds(pl.multiple_of(m * 16, 16), 16)
                total = (own[at, :].astype(F32) + E0[3, at, :].astype(F32)
                         + E2[0, at, :].astype(F32) + E2[1, at, :].astype(F32))
                DX[at, :] = total.astype(BF)
                return carry

            lax.fori_loop(0, tokens // 16, piece, 0)
            store(DX, dx_out)

        def finish_grads(p):
            two(p, 3)
            if p == 0:
                arrived(("g4", p), blocks(G, p, 2))
            for k in (0, 1):
                late = [R4[p].at[k, i] for i in (0, 1)] if p == 0 else []
                keep(p, k, R2[p].at[k, 0, 3], R2[p].at[k, 1, 3], *late)
            at = slice(base[p], base[p] + 3 * size[p])
            store(SUM.at[:, at], sum_out.at[:, at])

        finish_dx()
        s4(1)
        finish_grads(0)
        finish_grads(1)
        for p in (0, 1):
            left(p, blocks(W, p, 15))
            left(3 + p, blocks(G, p, 15))
        left(2, XQ.at[:, 0 : 7 * feats])
        left(5, PD.at[:, 0 : 7 * feats])
        for copy in stores:
            copy.wait()
        arrived(("g4", 1), blocks(G, 1, 2))

    count = 2 * (1 + 1 + 4 + 1) + 4 + 2 * (4 + 4 + 1 + 1) + 4 + 1 + 1
    n = [3 * h // 2 for h in size]
    scratch = [
        pltpu.VMEM((width, every), BF),
        pltpu.VMEM((2 * tokens, width), BF),
        pltpu.VMEM((tokens, every), F32),
        pltpu.VMEM((tokens, every), BF),
        pltpu.VMEM((width, every), BF),
        *[pltpu.VMEM((2, 2, SIDE, half, m), BF) for m in n],
        *[pltpu.VMEM((2, 2, SIDE, rows, m), BF) for m in n],
        *[pltpu.VMEM((2, 2, half, m), BF) for m in n],
        pltpu.VMEM((2, 2, rows, n[0]), BF),
        pltpu.VMEM((tokens, width), BF),
        pltpu.VMEM((SIDE, tokens, feats), BF),
        pltpu.VMEM((2, halftok, feats), BF),
        pltpu.VMEM((2, tokens, feats), BF),
        pltpu.VMEM((hidden, rows), BF),
        pltpu.VMEM((rows, every), F32),
        pltpu.VMEM((tokens, feats), BF),
        pltpu.SemaphoreType.DMA((7,)),
        pltpu.SemaphoreType.DMA((3,)),
        pltpu.SemaphoreType.DMA((6,)),
        pltpu.SemaphoreType.DMA((count,)),
    ]
    return kernel, scratch


def finish_of(rows, hidden):
    size, base = shares(hidden)
    n = 3 * size[1] // 2
    cut = n - size[1]

    def finish(dx_in, sum_in, late_in, dx_out, gate_out, up_out, down_out,
               DX, SUM, LATE, UP, GATE, DOWN, ins, outs):
        first = slice(0, base[1])
        last = slice(base[1], base[1] + 3 * size[1])
        loads = [
            pltpu.make_async_copy(sum_in.at[:, first], SUM.at[:, first], ins.at[0]),
            pltpu.make_async_copy(sum_in.at[:, last], SUM.at[:, last], ins.at[1]),
            pltpu.make_async_copy(late_in, LATE, ins.at[2]),
            pltpu.make_async_copy(dx_in, DX, ins.at[3]),
        ]
        for load in loads:
            load.start()
        h, at = size[0], base[1]
        stores = []

        def store(src, dst):
            copy = pltpu.make_async_copy(src, dst, outs.at[len(stores)])
            copy.start()
            stores.append(copy)

        loads[0].wait()
        store(SUM.at[:, 0:h], gate_out.at[:, 0:h])
        store(SUM.at[:, h : 2 * h], up_out.at[:, 0:h])
        DOWN[0:h, :] = SUM[:, 2 * h : 3 * h].T
        store(DOWN.at[0:h, :], down_out.at[0:h, :])
        loads[1].wait()
        loads[2].wait()
        total = [SUM[:, at + k * n : at + (k + 1) * n] + LATE[k, 0].astype(F32) + LATE[k, 1].astype(F32)
                 for k in (0, 1)]
        GATE[...] = total[0][:, 0 : size[1]]
        store(GATE, gate_out.at[:, h:hidden])
        UP[:, 0:cut] = total[0][:, size[1] : n]
        UP[:, cut : size[1]] = total[1][:, 0:cut]
        store(UP, up_out.at[:, h:hidden])
        DOWN[h:hidden, :] = total[1][:, cut:n].T
        store(DOWN.at[h:hidden, :], down_out.at[h:hidden, :])
        loads[3].wait()
        store(DX, dx_out)
        for copy in stores:
            copy.wait()

    return finish


def solution(mesh):
    def on_device(layer_input, out_cotangent, gate_matrix, up_matrix, down_matrix):
        tokens, feats = layer_input.shape
        rows, hidden = gate_matrix.shape
        width = feats * mesh.shape["tp"]
        kernel, scratch = kernel_of(rows, tokens, width, hidden)
        flops = 2 * 8 * tokens * width * hidden
        late = (2, 2, rows, shares(hidden)[0][1] * 3 // 2)
        any_space = pl.BlockSpec(memory_space=pl.ANY)
        dx, sums, lates = pl.pallas_call(
            kernel,
            out_shape=(
                jax.ShapeDtypeStruct((tokens, feats), BF),
                jax.ShapeDtypeStruct((rows, 3 * hidden), F32),
                jax.ShapeDtypeStruct(late, BF),
            ),
            in_specs=[any_space] * 5,
            out_specs=[any_space] * 3,
            scratch_shapes=scratch,
            compiler_params=pltpu.CompilerParams(
                collective_id=0, has_side_effects=True, vmem_limit_bytes=66_000_000),
            cost_estimate=pl.CostEstimate(
                flops=flops, bytes_accessed=4 << 20, transcendentals=tokens * hidden),
        )(layer_input, out_cotangent, gate_matrix, up_matrix, down_matrix)
        return pl.pallas_call(
            finish_of(rows, hidden),
            out_shape=(
                jax.ShapeDtypeStruct((tokens, feats), BF),
                jax.ShapeDtypeStruct((rows, hidden), F32),
                jax.ShapeDtypeStruct((rows, hidden), F32),
                jax.ShapeDtypeStruct((hidden, rows), F32),
            ),
            in_specs=[any_space] * 3,
            out_specs=[any_space] * 4,
            scratch_shapes=[
                pltpu.VMEM((tokens, feats), BF),
                pltpu.VMEM((rows, 3 * hidden), F32),
                pltpu.VMEM(late, BF),
                pltpu.VMEM((rows, shares(hidden)[0][1]), F32),
                pltpu.VMEM((rows, shares(hidden)[0][1]), F32),
                pltpu.VMEM((hidden, rows), F32),
                pltpu.SemaphoreType.DMA((4,)),
                pltpu.SemaphoreType.DMA((7,)),
            ],
        )(dx, sums, lates)

    return jax.shard_map(
        on_device, mesh=mesh,
        in_specs=(P("fs", "tp"), P("fs", "tp"), P("fs", "tp"), P("fs", "tp"), P("tp", "fs")),
        out_specs=(P("fs", "tp"), P("fs", "tp"), P("fs", "tp"), P("tp", "fs")),
        check_vma=False)
```

```python
import jax
import jax.numpy as jnp
from jax import lax
from jax.experimental import pallas as pl
from jax.experimental.pallas import tpu as pltpu
from jax.sharding import PartitionSpec as P

MESH = pl.DeviceIdType.MESH
BF = jnp.bfloat16
F32 = jnp.float32
SIDE = 4
ORDER = (2, 1, -1, 0)


def shares(hidden):
    first = 2 * hidden // 3
    return (first, hidden - first), (0, 3 * first)


def kernel_of(rows, tokens, width, hidden):
    size, base = shares(hidden)
    half = rows // 2
    feats = width // 8
    band = SIDE * rows
    halftok = tokens // 2
    every = 3 * hidden

    def kernel(x_in, q_in, gate_in, up_in, down_in, dx_out, sum_out, late_out,
               W, XQ, ACC, D, G, R1a, R1b, R2a, R2b, R3a, R3b, R4a, PD, E0, E1, E2, DN, SUM, DX,
               load_sem, ss, rs):
        R1, R2, R3, R4 = (R1a, R1b), (R2a, R2b), (R3a, R3b), (R4a, late_out)
        fs, tp = lax.axis_index("fs"), lax.axis_index("tp")
        z, y = fs // SIDE, fs % SIDE
        x, c = tp // 2, tp % 2

        def turn(a, o):
            return (a + (o % SIDE)) % SIDE

        def fs_dev(f):
            return {"fs": f, "tp": tp}

        def tp_dev(t):
            return {"fs": fs, "tp": t}

        def big_dev(k, d):
            return fs_dev(turn(z, d) * SIDE + y) if k == 0 else fs_dev(z * SIDE + turn(y, d))

        def small_dev(k, d):
            return big_dev(1 - k, d)

        sibling = tp_dev(x * 2 + (1 - c))

        def x_dev(d):
            return tp_dev(turn(x, d) * 2 + c)

        barrier = pltpu.get_barrier_semaphore()
        for partner in (big_dev(0, 1), big_dev(0, -1), big_dev(1, 1), big_dev(1, -1),
                        x_dev(1), x_dev(-1), sibling):
            pl.semaphore_signal(barrier, inc=1, device_id=partner, device_id_type=MESH)
        mine = pl.ds(pl.multiple_of(fs * rows, rows), rows)
        my_feats = pl.ds(pl.multiple_of(tp * feats, feats), feats)
        loads = []

        def load(src, dst):
            copy = pltpu.make_async_copy(src, dst, load_sem.at[len(loads)])
            copy.start()
            loads.append(copy)

        for p in (0, 1):
            at, h, from_ = base[p], size[p], p * size[0]
            for i, ref in enumerate((gate_in, up_in)):
                load(ref.at[:, from_ : from_ + h], W.at[mine, at + i * h : at + (i + 1) * h])
            if p == 0:
                load(down_in, DN)
                load(x_in, XQ.at[0:tokens, my_feats])
                load(q_in, XQ.at[tokens : 2 * tokens, my_feats])

        def turn_down():
            loads[2].wait()
            turned = DN[...].astype(F32).T.astype(BF)
            for p in (0, 1):
                at, h, from_ = base[p], size[p], p * size[0]
                W[mine, at + 2 * h : at + 3 * h] = turned[:, from_ : from_ + h]

        def meet():
            pl.semaphore_wait(barrier, 7)

        meet()

        slots, again = {}, {}
        for p in (0, 1):
            for j, r in enumerate(ORDER):
                again["g1", p, j] = "a3", p, r
            again["g2", p, 0] = "a4", p
            again["g2", p, 2] = "g2", p, 1
            again["g3", p] = "a1", p
            again["g4", p] = "a2", p

        def slot(name):
            name = again.get(name, name)
            if name not in slots:
                slots[name] = len(slots)
            return slots[name]

        def send(group, name, src, dst, dev):
            pltpu.make_async_remote_copy(
                src_ref=src, dst_ref=dst, send_sem=ss.at[group], recv_sem=rs.at[slot(name)],
                device_id=dev, device_id_type=MESH).start()

        def awaited(name, like):
            return pltpu.make_async_remote_copy(
                src_ref=like, dst_ref=like, send_sem=ss.at[0], recv_sem=rs.at[slot(name)],
                device_id=sibling, device_id_type=MESH)

        def arrived(name, like):
            awaited(name, like).wait_recv()

        def left(group, like):
            pltpu.make_async_remote_copy(
                src_ref=like, dst_ref=like, send_sem=ss.at[group], recv_sem=rs.at[0],
                device_id=sibling, device_id_type=MESH).wait_send()

        def block(k, so, bo, part=None):
            zo, yo = (bo, so) if k == 0 else (so, bo)
            start = (turn(z, zo) * SIDE + turn(y, yo)) * rows
            if part is None:
                return pl.ds(pl.multiple_of(start, rows), rows)
            return pl.ds(pl.multiple_of(start + part * half, half), half)

        def lanes(p, k):
            cols = 3 * size[p] // 2
            return slice(base[p] + k * cols, base[p] + (k + 1) * cols)

        def blocks(ref, p, n):
            return ref.at[0 : n * rows, base[p] : base[p] + 3 * size[p]]

        def w(p, k, so, bo, part=None):
            return W.at[block(k, so, bo, part), lanes(p, k)]

        def near(p, k):
            for d in (1, -1):
                send(0, ("a1", p), w(p, k, 0, 0), w(p, k, 0, 0), small_dev(k, d))

        def far(p, r):
            for k in (0, 1):
                for d in (1, -1):
                    send(0, ("a3", p, r), w(p, k, r, 0), w(p, k, r, 0), big_dev(k, d))

        def near_arrived(p):
            arrived(("a1", p), blocks(W, p, 2))
            for k in (0, 1):
                for i, d in enumerate((1, -1)):
                    send(0, ("a2", p), w(p, k, -d, 0, i), w(p, k, -d, 0, i), small_dev(k, d))

        def opposite_arrived(p):
            arrived(("a2", p), blocks(W, p, 1))

        def far_arrived(p, r):
            arrived(("a3", p, r), blocks(W, p, 2))
            for k in (0, 1):
                for i, d in enumerate((1, -1)):
                    send(0, ("a4", p), w(p, k, r, -d, i), w(p, k, r, -d, i), big_dev(k, d))

        def last_arrived(p):
            arrived(("a4", p), blocks(W, p, 4))

        def xq(xo, core, part):
            start = (turn(x, xo) * 2 + core) * feats
            lane = pl.ds(pl.multiple_of(start, feats), feats)
            return XQ.at[part * tokens : (part + 1) * tokens, lane]

        def x_own(i):
            for d in (1, -1):
                part = i if d == 1 else 1 - i
                send(2, ("x1", i), xq(0, c, part), xq(0, c, part), x_dev(d))

        def to_sibling(xo, part):
            send(2, "sib", xq(xo, c, part), xq(xo, c, part), sibling)

        def x_first():
            arrived(("x1", 0), XQ.at[:, 0:feats])
            for i, d in enumerate((1, -1)):
                send(2, "x2", xq(-d, c, i), xq(-d, c, i), x_dev(d))
            for i, d in enumerate((1, -1)):
                to_sibling(-d, i)

        def x_second():
            arrived(("x1", 1), XQ.at[:, 0:feats])
            for i, d in enumerate((1, -1)):
                to_sibling(-d, 1 - i)

        def x_third():
            arrived("x2", XQ.at[:, 0:feats])
            for i in (0, 1):
                to_sibling(2, i)

        def x_last():
            arrived("sib", XQ.at[:, 0 : 4 * feats])

        loads[0].wait()
        loads[1].wait()
        near(0, 0)
        turn_down()
        near(0, 1)
        far(0, 0)
        loads[3].wait()
        loads[4].wait()
        x_own(0)
        x_own(1)
        for part in (0, 1):
            to_sibling(0, part)
        loads[5].wait()
        loads[6].wait()
        for k in (0, 1):
            near(1, k)

        near_arrived(0)
        for r in (1, -1):
            far(0, r)
        x_first()
        far_arrived(0, 0)
        near_arrived(1)
        opposite_arrived(0)
        far(0, 2)
        far_arrived(0, 1)
        x_second()
        far_arrived(0, -1)
        far(1, 0)
        x_third()
        far_arrived(0, 2)
        for r in (1, -1):
            far(1, r)
        opposite_arrived(1)
        far(1, 2)
        x_last()

        tile = tokens // 3

        def dot(a, b, dims):
            return lax.dot_general(a, b, (dims, ((), ())), preferred_element_type=F32)

        def put(at, lane, value, first):
            if first:
                ACC[at, lane] = value
            else:
                ACC[at, lane] += value

        def forward(p, k, o, first=False):
            both = lanes(p, k)
            split = base[p] + 2 * size[p]

            def piece(m, carry):
                at = pl.ds(pl.multiple_of(m * tile, tile), tile)
                low = pl.ds(pl.multiple_of(tokens + m * tile, tile), tile)
                if k == 0:
                    span = pl.ds(pl.multiple_of(turn(z, o) * band, band), band)
                    put(at, both, dot(XQ[at, span], W[span, both], ((1,), (0,))), first)
                else:
                    spans = [pl.ds(pl.multiple_of(i * band + turn(y, o) * rows, rows), rows)
                             for i in range(SIDE)]
                    for top, lane in ((at, slice(both.start, split)), (low, slice(split, both.stop))):
                        a = jnp.concatenate([XQ[top, s] for s in spans], axis=1)
                        b = jnp.concatenate([W[s, lane] for s in spans], axis=0)
                        put(at, lane, dot(a, b, ((1,), (0,))), first)
                return carry
            lax.fori_loop(0, 3, piece, 0)

        step = tokens // 24

        def gate(p):
            h = size[p]
            one, two, three, four = (base[p] + i * h for i in range(4))

            def piece(m, carry):
                at = pl.ds(pl.multiple_of(m * step, step), step)
                g = ACC[at, one:two]
                u = ACC[at, two:three]
                e = ACC[at, three:four]
                s = 1.0 / (1.0 + jnp.exp(-g))
                act = g * s
                D[at, one:two] = (e * u * s * (1.0 + g * (1.0 - s))).astype(BF)
                D[at, two:three] = (e * act).astype(BF)
                D[at, three:four] = (act * u).astype(BF)
                return carry

            lax.fori_loop(0, 24, piece, 0)

        def grads(p, k, o):
            both = lanes(p, k)
            split = base[p] + 2 * size[p]

            def piece(n, carry):
                if k == 0:
                    span = pl.ds(pl.multiple_of(turn(z, o) * band + n * 2 * rows, 2 * rows), 2 * rows)
                    G[span, both] = dot(XQ[0:tokens, span], D[:, both], ((0,), (0,))).astype(BF)
                else:
                    spans = [pl.ds(pl.multiple_of((2 * n + i) * band + turn(y, o) * rows, rows), rows)
                             for i in range(2)]
                    for top, lane in ((0, slice(both.start, split)), (tokens, slice(split, both.stop))):
                        a = jnp.concatenate([XQ[top : top + tokens, s] for s in spans], axis=1)
                        r = dot(a, D[:, lane], ((0,), (0,))).astype(BF)
                        for i in range(2):
                            G[spans[i], lane] = r[i * rows : (i + 1) * rows]
                return carry
            lax.fori_loop(0, 2, piece, 0)

        def g(p, k, so, bo, part=None):
            return G.at[block(k, so, bo, part), lanes(p, k)]

        def add_into(ref, *others):
            def piece(m, carry):
                at = pl.ds(pl.multiple_of(m * 16, 16), 16)
                total = ref[at, :].astype(F32)
                for other in others:
                    total = total + other[at, :].astype(F32)
                ref[at, :] = total.astype(BF)
                return carry
            lax.fori_loop(0, ref.shape[0] // 16, piece, 0)

        def s1(p):
            for j, r in enumerate(ORDER):
                for k in (0, 1):
                    for i, d in enumerate((1, -1)):
                        send(1, ("g1", p, j), g(p, k, r, 2, i), R1[p].at[k, i, j],
                             big_dev(k, d))

        def s2(p, j):
            r = ORDER[j]
            arrived(("g1", p, j), blocks(G, p, 1))
            for k in (0, 1):
                for i, d in enumerate((1, -1)):
                    add_into(g(p, k, r, d, i), R1[p].at[k, i, j])
            for k in (0, 1):
                for i, d in enumerate((1, -1)):
                    send(1, ("g2", p, j), g(p, k, r, d), R2[p].at[k, i, j], big_dev(k, d))

        def two(p, j):
            arrived(("g2", p, j), blocks(G, p, 2))

        def s3(p):
            two(p, 0)
            for k in (0, 1):
                add_into(g(p, k, 2, 0), R2[p].at[k, 0, 0], R2[p].at[k, 1, 0])
            for k in (0, 1):
                for i, d in enumerate((1, -1)):
                    send(1, ("g3", p), g(p, k, 2, 0, i), R3[p].at[k, i], small_dev(k, d))

        def pre4(p):
            arrived(("g2", p, 1), blocks(G, p, 4))
            for i, d in enumerate((1, -1)):
                for k in (0, 1):
                    add_into(g(p, k, d, 0), R2[p].at[k, 0, 1 + i], R2[p].at[k, 1, 1 + i])

        def s4(p):
            arrived(("g3", p), blocks(G, p, 1))
            for k in (0, 1):
                for i, d in enumerate((1, -1)):
                    add_into(g(p, k, d, 0, i), R3[p].at[k, i])
            for k in (0, 1):
                for i, d in enumerate((1, -1)):
                    send(1, ("g4", p), g(p, k, d, 0), R4[p].at[k, i], small_dev(k, d))

        def keep(p, k, *others):
            own, to = g(p, k, 0, 0), SUM.at[:, lanes(p, k)]

            def piece(m, carry):
                at = pl.ds(pl.multiple_of(m * 16, 16), 16)
                total = own[at, :].astype(F32)
                for other in others:
                    total = total + other[at, :].astype(F32)
                to[at, :] = total
                return carry

            lax.fori_loop(0, rows // 16, piece, 0)

        def partial_of(xo, core):
            start = (turn(x, xo) * 2 + core) * feats
            span = pl.ds(pl.multiple_of(start, feats), feats)

            def piece(m, carry):
                at = pl.ds(pl.multiple_of(m * tile, tile), tile)
                total = 0.0
                for p in (0, 1):
                    lane = slice(base[p], base[p] + 2 * size[p])
                    total = total + dot(D[at, lane], W[span, lane], ((1,), (1,)))
                PD[at, span] = total.astype(BF)
                return carry
            lax.fori_loop(0, 3, piece, 0)

        def pd(xo, core, part=None):
            start = (turn(x, xo) * 2 + core) * feats
            lane = pl.ds(pl.multiple_of(start, feats), feats)
            if part is None:
                return PD.at[:, lane]
            return PD.at[part * halftok : (part + 1) * halftok, lane]

        for o in (0, 1, -1):
            for k in (0, 1):
                forward(0, k, o, o == 0)
        far_arrived(1, 0)
        last_arrived(0)
        for k in (0, 1):
            forward(0, k, 2)
        gate(0)
        far_arrived(1, 1)
        far_arrived(1, -1)
        for k in (0, 1):
            grads(0, k, 2)
        far_arrived(1, 2)
        s1(0)
        for o in (1, -1):
            for k in (0, 1):
                grads(0, k, o)

        for j, o in enumerate((0, 1, -1)):
            for k in (0, 1):
                forward(1, k, o, o == 0)
            s2(0, j)
        last_arrived(1)
        for k in (0, 1):
            forward(1, k, 2)
        gate(1)
        for k in (0, 1):
            grads(1, k, 2)
        s1(1)
        for o in (1, -1):
            for k in (0, 1):
                grads(1, k, o)
        for k in (0, 1):
            grads(0, k, 0)
        s3(0)
        s2(0, 3)
        for j, r in enumerate(ORDER):
            partial_of(r, 1 - c)
            send(3, "d0", pd(r, 1 - c), E0.at[j], sibling)

        def sibling_sum(j):
            add_into(pd(ORDER[j], c), E0.at[j])

        partial_of(2, c)
        arrived("d0", PD.at[:, 0 : 4 * feats])
        sibling_sum(0)
        for i, d in enumerate((1, -1)):
            send(3, "d1", pd(2, c, i), E1.at[i], x_dev(d))
        for j in (1, 2):
            partial_of(ORDER[j], c)
            sibling_sum(j)
        for j in (0, 1, 2):
            s2(1, j)
        pre4(0)
        partial_of(0, c)
        s4(0)
        arrived("d1", PD.at[:, 0:feats])
        for i, d in enumerate((1, -1)):
            add_into(pd(d, c, i), E1.at[i])
            send(3, "d2", pd(d, c), E2.at[i], x_dev(d))
        for k in (0, 1):
            grads(1, k, 0)
        s3(1)
        s2(1, 3)
        pre4(1)

        stores = []

        def store(src, dst):
            copy = pltpu.make_async_copy(src, dst, load_sem.at[len(stores)])
            copy.start()
            stores.append(copy)

        def finish_dx():
            arrived("d2", PD.at[:, 0 : 2 * feats])
            own = pd(0, c)

            def piece(m, carry):
                at = pl.ds(pl.multiple_of(m * 16, 16), 16)
                total = (own[at, :].astype(F32) + E0[3, at, :].astype(F32)
                         + E2[0, at, :].astype(F32) + E2[1, at, :].astype(F32))
                DX[at, :] = total.astype(BF)
                return carry

            lax.fori_loop(0, tokens // 16, piece, 0)
            store(DX, dx_out)

        def finish_grads(p):
            two(p, 3)
            if p == 0:
                arrived(("g4", p), blocks(G, p, 2))
            for k in (0, 1):
                late = [R4[p].at[k, i] for i in (0, 1)] if p == 0 else []
                keep(p, k, R2[p].at[k, 0, 3], R2[p].at[k, 1, 3], *late)
            at = slice(base[p], base[p] + 3 * size[p])
            store(SUM.at[:, at], sum_out.at[:, at])

        finish_dx()
        s4(1)
        finish_grads(0)
        finish_grads(1)
        left(0, W.at[0 : 15 * rows, :])
        left(1, G.at[0 : 15 * rows, :])
        left(2, XQ.at[:, 0 : 7 * feats])
        left(3, PD.at[:, 0 : 7 * feats])
        for copy in stores:
            copy.wait()
        arrived(("g4", 1), blocks(G, 1, 2))

    count = 2 * (1 + 1 + 4 + 1) + 4 + 2 * 2 + 1 + 1 + 1
    n = [3 * h // 2 for h in size]
    scratch = [
        pltpu.VMEM((width, every), BF),
        pltpu.VMEM((2 * tokens, width), BF),
        pltpu.VMEM((tokens, every), F32),
        pltpu.VMEM((tokens, every), BF),
        pltpu.VMEM((width, every), BF),
        *[pltpu.VMEM((2, 2, SIDE, half, m), BF) for m in n],
        *[pltpu.VMEM((2, 2, SIDE, rows, m), BF) for m in n],
        *[pltpu.VMEM((2, 2, half, m), BF) for m in n],
        pltpu.VMEM((2, 2, rows, n[0]), BF),
        pltpu.VMEM((tokens, width), BF),
        pltpu.VMEM((SIDE, tokens, feats), BF),
        pltpu.VMEM((2, halftok, feats), BF),
        pltpu.VMEM((2, tokens, feats), BF),
        pltpu.VMEM((hidden, rows), BF),
        pltpu.VMEM((rows, every), F32),
        pltpu.VMEM((tokens, feats), BF),
        pltpu.SemaphoreType.DMA((7,)),
        pltpu.SemaphoreType.DMA((4,)),
        pltpu.SemaphoreType.DMA((count,)),
    ]
    return kernel, scratch


def finish_of(rows, hidden):
    size, base = shares(hidden)
    n = 3 * size[1] // 2
    cut = n - size[1]

    def finish(dx_in, sum_in, late_in, dx_out, gate_out, up_out, down_out,
               DX, SUM, LATE, UP, GATE, DOWN, ins, outs):
        first = slice(0, base[1])
        last = slice(base[1], base[1] + 3 * size[1])
        loads = [
            pltpu.make_async_copy(sum_in.at[:, first], SUM.at[:, first], ins.at[0]),
            pltpu.make_async_copy(sum_in.at[:, last], SUM.at[:, last], ins.at[1]),
            pltpu.make_async_copy(late_in, LATE, ins.at[2]),
            pltpu.make_async_copy(dx_in, DX, ins.at[3]),
        ]
        for load in loads:
            load.start()
        h, at = size[0], base[1]
        stores = []

        def store(src, dst):
            copy = pltpu.make_async_copy(src, dst, outs.at[len(stores)])
            copy.start()
            stores.append(copy)

        loads[0].wait()
        store(SUM.at[:, 0:h], gate_out.at[:, 0:h])
        store(SUM.at[:, h : 2 * h], up_out.at[:, 0:h])
        DOWN[0:h, :] = SUM[:, 2 * h : 3 * h].T
        store(DOWN.at[0:h, :], down_out.at[0:h, :])
        loads[1].wait()
        loads[2].wait()
        total = [SUM[:, at + k * n : at + (k + 1) * n] + LATE[k, 0].astype(F32) + LATE[k, 1].astype(F32)
                 for k in (0, 1)]
        GATE[...] = total[0][:, 0 : size[1]]
        store(GATE, gate_out.at[:, h:hidden])
        UP[:, 0:cut] = total[0][:, size[1] : n]
        UP[:, cut : size[1]] = total[1][:, 0:cut]
        store(UP, up_out.at[:, h:hidden])
        DOWN[h:hidden, :] = total[1][:, cut:n].T
        store(DOWN.at[h:hidden, :], down_out.at[h:hidden, :])
        loads[3].wait()
        store(DX, dx_out)
        for copy in stores:
            copy.wait()

    return finish


def solution(mesh):
    def on_device(layer_input, out_cotangent, gate_matrix, up_matrix, down_matrix):
        tokens, feats = layer_input.shape
        rows, hidden = gate_matrix.shape
        width = feats * mesh.shape["tp"]
        kernel, scratch = kernel_of(rows, tokens, width, hidden)
        flops = 2 * 8 * tokens * width * hidden
        late = (2, 2, rows, shares(hidden)[0][1] * 3 // 2)
        any_space = pl.BlockSpec(memory_space=pl.ANY)
        dx, sums, lates = pl.pallas_call(
            kernel,
            out_shape=(
                jax.ShapeDtypeStruct((tokens, feats), BF),
                jax.ShapeDtypeStruct((rows, 3 * hidden), F32),
                jax.ShapeDtypeStruct(late, BF),
            ),
            in_specs=[any_space] * 5,
            out_specs=[any_space] * 3,
            scratch_shapes=scratch,
            compiler_params=pltpu.CompilerParams(
                collective_id=0, has_side_effects=True, vmem_limit_bytes=66_000_000),
            cost_estimate=pl.CostEstimate(
                flops=flops, bytes_accessed=4 << 20, transcendentals=tokens * hidden),
        )(layer_input, out_cotangent, gate_matrix, up_matrix, down_matrix)
        return pl.pallas_call(
            finish_of(rows, hidden),
            out_shape=(
                jax.ShapeDtypeStruct((tokens, feats), BF),
                jax.ShapeDtypeStruct((rows, hidden), F32),
                jax.ShapeDtypeStruct((rows, hidden), F32),
                jax.ShapeDtypeStruct((hidden, rows), F32),
            ),
            in_specs=[any_space] * 3,
            out_specs=[any_space] * 4,
            scratch_shapes=[
                pltpu.VMEM((tokens, feats), BF),
                pltpu.VMEM((rows, 3 * hidden), F32),
                pltpu.VMEM(late, BF),
                pltpu.VMEM((rows, shares(hidden)[0][1]), F32),
                pltpu.VMEM((rows, shares(hidden)[0][1]), F32),
                pltpu.VMEM((hidden, rows), F32),
                pltpu.SemaphoreType.DMA((4,)),
                pltpu.SemaphoreType.DMA((7,)),
            ],
        )(dx, sums, lates)

    return jax.shard_map(
        on_device, mesh=mesh,
        in_specs=(P("fs", "tp"), P("fs", "tp"), P("fs", "tp"), P("fs", "tp"), P("tp", "fs")),
        out_specs=(P("fs", "tp"), P("fs", "tp"), P("fs", "tp"), P("tp", "fs")),
        check_vma=False)
```

```python
import jax
import jax.numpy as jnp
from jax import lax
from jax.experimental import pallas as pl
from jax.experimental.pallas import tpu as pltpu
from jax.sharding import PartitionSpec as P

MESH = pl.DeviceIdType.MESH
BF = jnp.bfloat16
F32 = jnp.float32
SIDE = 4
ORDER = (2, 1, -1, 0)


def shares(hidden):
    first = 2 * hidden // 3
    return (first, hidden - first), (0, 3 * first)


def kernel_of(rows, tokens, width, hidden):
    size, base = shares(hidden)
    half = rows // 2
    feats = width // 8
    band = SIDE * rows
    halftok = tokens // 2
    every = 3 * hidden

    def kernel(x_in, q_in, gate_in, up_in, down_in, dx_out, sum_out, late_out,
               W, XQ, ACC, D, G, R1a, R1b, R2a, R2b, R3a, R3b, R4a, PD, E0, E1, E2, DN, SUM, DX,
               load_sem, ss, rs):
        R1, R2, R3, R4 = (R1a, R1b), (R2a, R2b), (R3a, R3b), (R4a, late_out)
        fs, tp = lax.axis_index("fs"), lax.axis_index("tp")
        z, y = fs // SIDE, fs % SIDE
        x, c = tp // 2, tp % 2

        def turn(a, o):
            return (a + (o % SIDE)) % SIDE

        def fs_dev(f):
            return {"fs": f, "tp": tp}

        def tp_dev(t):
            return {"fs": fs, "tp": t}

        def big_dev(k, d):
            return fs_dev(turn(z, d) * SIDE + y) if k == 0 else fs_dev(z * SIDE + turn(y, d))

        def small_dev(k, d):
            return big_dev(1 - k, d)

        sibling = tp_dev(x * 2 + (1 - c))

        def x_dev(d):
            return tp_dev(turn(x, d) * 2 + c)

        barrier = pltpu.get_barrier_semaphore()
        for partner in (big_dev(0, 1), big_dev(0, -1), big_dev(1, 1), big_dev(1, -1),
                        x_dev(1), x_dev(-1), sibling):
            pl.semaphore_signal(barrier, inc=1, device_id=partner, device_id_type=MESH)
        mine = pl.ds(pl.multiple_of(fs * rows, rows), rows)
        my_feats = pl.ds(pl.multiple_of(tp * feats, feats), feats)
        def load(group, src, dst):
            pltpu.make_async_copy(src, dst, load_sem.at[group]).start()

        def loaded(group, like):
            pltpu.make_async_copy(like, like, load_sem.at[group]).wait()

        for p in (0, 1):
            at, h, from_ = base[p], size[p], p * size[0]
            for i, ref in enumerate((gate_in, up_in)):
                load(3 * p, ref.at[:, from_ : from_ + h],
                     W.at[mine, at + i * h : at + (i + 1) * h])
            if p == 0:
                load(1, down_in, DN)
                load(2, x_in, XQ.at[0:tokens, my_feats])
                load(2, q_in, XQ.at[tokens : 2 * tokens, my_feats])

        def turn_down():
            loaded(1, DN)
            turned = DN[...].astype(F32).T.astype(BF)
            for p in (0, 1):
                at, h, from_ = base[p], size[p], p * size[0]
                W[mine, at + 2 * h : at + 3 * h] = turned[:, from_ : from_ + h]

        def meet():
            pl.semaphore_wait(barrier, 7)

        meet()

        slots, again = {}, {}
        for p in (0, 1):
            for j, r in enumerate(ORDER):
                again["g1", p, j] = "a3", p, r
            again["g2", p, 0] = "a4", p
            again["g2", p, 2] = "g2", p, 1
            again["g3", p] = "a1", p
            again["g4", p] = "a2", p
        again["g2", 1, 1] = again["g2", 1, 2] = "a3", 0, ORDER[0]
        again["g2", 1, 3] = "a3", 0, ORDER[1]
        again["d0"] = "x1", 0

        def slot(name):
            name = again.get(name, name)
            if name not in slots:
                slots[name] = len(slots)
            return slots[name]

        def send(group, name, src, dst, dev):
            pltpu.make_async_remote_copy(
                src_ref=src, dst_ref=dst, send_sem=ss.at[group], recv_sem=rs.at[slot(name)],
                device_id=dev, device_id_type=MESH).start()

        def awaited(name, like):
            return pltpu.make_async_remote_copy(
                src_ref=like, dst_ref=like, send_sem=ss.at[0], recv_sem=rs.at[slot(name)],
                device_id=sibling, device_id_type=MESH)

        def arrived(name, like):
            awaited(name, like).wait_recv()

        def left(group, like):
            pltpu.make_async_remote_copy(
                src_ref=like, dst_ref=like, send_sem=ss.at[group], recv_sem=rs.at[0],
                device_id=sibling, device_id_type=MESH).wait_send()

        def block(k, so, bo, part=None):
            zo, yo = (bo, so) if k == 0 else (so, bo)
            start = (turn(z, zo) * SIDE + turn(y, yo)) * rows
            if part is None:
                return pl.ds(pl.multiple_of(start, rows), rows)
            return pl.ds(pl.multiple_of(start + part * half, half), half)

        def lanes(p, k):
            cols = 3 * size[p] // 2
            return slice(base[p] + k * cols, base[p] + (k + 1) * cols)

        def blocks(ref, p, n):
            return ref.at[0 : n * rows, base[p] : base[p] + 3 * size[p]]

        def w(p, k, so, bo, part=None):
            return W.at[block(k, so, bo, part), lanes(p, k)]

        def near(p, k):
            for d in (1, -1):
                send(0, ("a1", p), w(p, k, 0, 0), w(p, k, 0, 0), small_dev(k, d))

        def far(p, r):
            for k in (0, 1):
                for d in (1, -1):
                    send(0, ("a3", p, r), w(p, k, r, 0), w(p, k, r, 0), big_dev(k, d))

        def near_arrived(p):
            arrived(("a1", p), blocks(W, p, 2))
            for k in (0, 1):
                for i, d in enumerate((1, -1)):
                    send(0, ("a2", p), w(p, k, -d, 0, i), w(p, k, -d, 0, i), small_dev(k, d))

        def opposite_arrived(p):
            arrived(("a2", p), blocks(W, p, 1))

        def far_arrived(p, r):
            arrived(("a3", p, r), blocks(W, p, 2))
            for k in (0, 1):
                for i, d in enumerate((1, -1)):
                    send(0, ("a4", p), w(p, k, r, -d, i), w(p, k, r, -d, i), big_dev(k, d))

        def last_arrived(p):
            arrived(("a4", p), blocks(W, p, 4))

        def xq(xo, core, part):
            start = (turn(x, xo) * 2 + core) * feats
            lane = pl.ds(pl.multiple_of(start, feats), feats)
            return XQ.at[part * tokens : (part + 1) * tokens, lane]

        def x_own(i):
            for d in (1, -1):
                part = i if d == 1 else 1 - i
                send(2, ("x1", i), xq(0, c, part), xq(0, c, part), x_dev(d))

        def to_sibling(xo, part):
            send(2, "sib", xq(xo, c, part), xq(xo, c, part), sibling)

        def x_first():
            arrived(("x1", 0), XQ.at[:, 0:feats])
            for i, d in enumerate((1, -1)):
                send(2, "x2", xq(-d, c, i), xq(-d, c, i), x_dev(d))
            for i, d in enumerate((1, -1)):
                to_sibling(-d, i)

        def x_second():
            arrived(("x1", 1), XQ.at[:, 0:feats])
            for i, d in enumerate((1, -1)):
                to_sibling(-d, 1 - i)

        def x_third():
            arrived("x2", XQ.at[:, 0:feats])
            for i in (0, 1):
                to_sibling(2, i)

        def x_last():
            arrived("sib", XQ.at[:, 0 : 4 * feats])

        loaded(0, W.at[mine, 0 : 2 * size[0]])
        near(0, 0)
        turn_down()
        near(0, 1)
        far(0, 0)
        loaded(2, XQ.at[:, my_feats])
        x_own(0)
        x_own(1)
        for part in (0, 1):
            to_sibling(0, part)
        loaded(3, W.at[mine, base[1] : base[1] + 2 * size[1]])
        for k in (0, 1):
            near(1, k)

        near_arrived(0)
        for r in (1, -1):
            far(0, r)
        x_first()
        far_arrived(0, 0)
        near_arrived(1)
        opposite_arrived(0)
        far(0, 2)
        far_arrived(0, 1)
        x_second()
        far_arrived(0, -1)
        far(1, 0)
        x_third()
        far_arrived(0, 2)
        for r in (1, -1):
            far(1, r)
        opposite_arrived(1)
        far(1, 2)
        x_last()

        tile = tokens // 3

        def dot(a, b, dims):
            return lax.dot_general(a, b, (dims, ((), ())), preferred_element_type=F32)

        def put(at, lane, value, first):
            if first:
                ACC[at, lane] = value
            else:
                ACC[at, lane] += value

        def forward(p, k, o, first=False):
            both = lanes(p, k)
            split = base[p] + 2 * size[p]

            def piece(m, carry):
                at = pl.ds(pl.multiple_of(m * tile, tile), tile)
                low = pl.ds(pl.multiple_of(tokens + m * tile, tile), tile)
                if k == 0:
                    span = pl.ds(pl.multiple_of(turn(z, o) * band, band), band)
                    put(at, both, dot(XQ[at, span], W[span, both], ((1,), (0,))), first)
                else:
                    spans = [pl.ds(pl.multiple_of(i * band + turn(y, o) * rows, rows), rows)
                             for i in range(SIDE)]
                    for top, lane in ((at, slice(both.start, split)), (low, slice(split, both.stop))):
                        a = jnp.concatenate([XQ[top, s] for s in spans], axis=1)
                        b = jnp.concatenate([W[s, lane] for s in spans], axis=0)
                        put(at, lane, dot(a, b, ((1,), (0,))), first)
                return carry
            lax.fori_loop(0, 3, piece, 0)

        step = tokens // 24

        def gate(p):
            h = size[p]
            one, two, three, four = (base[p] + i * h for i in range(4))

            def piece(m, carry):
                at = pl.ds(pl.multiple_of(m * step, step), step)
                g = ACC[at, one:two]
                u = ACC[at, two:three]
                e = ACC[at, three:four]
                s = 1.0 / (1.0 + jnp.exp(-g))
                act = g * s
                D[at, one:two] = (e * u * s * (1.0 + g * (1.0 - s))).astype(BF)
                D[at, two:three] = (e * act).astype(BF)
                D[at, three:four] = (act * u).astype(BF)
                return carry

            lax.fori_loop(0, 24, piece, 0)

        def grads(p, k, o):
            both = lanes(p, k)
            split = base[p] + 2 * size[p]

            def piece(n, carry):
                if k == 0:
                    span = pl.ds(pl.multiple_of(turn(z, o) * band + n * 2 * rows, 2 * rows), 2 * rows)
                    G[span, both] = dot(XQ[0:tokens, span], D[:, both], ((0,), (0,))).astype(BF)
                else:
                    spans = [pl.ds(pl.multiple_of((2 * n + i) * band + turn(y, o) * rows, rows), rows)
                             for i in range(2)]
                    for top, lane in ((0, slice(both.start, split)), (tokens, slice(split, both.stop))):
                        a = jnp.concatenate([XQ[top : top + tokens, s] for s in spans], axis=1)
                        r = dot(a, D[:, lane], ((0,), (0,))).astype(BF)
                        for i in range(2):
                            G[spans[i], lane] = r[i * rows : (i + 1) * rows]
                return carry
            lax.fori_loop(0, 2, piece, 0)

        def g(p, k, so, bo, part=None):
            return G.at[block(k, so, bo, part), lanes(p, k)]

        def add_into(ref, *others):
            def piece(m, carry):
                at = pl.ds(pl.multiple_of(m * 16, 16), 16)
                total = ref[at, :].astype(F32)
                for other in others:
                    total = total + other[at, :].astype(F32)
                ref[at, :] = total.astype(BF)
                return carry
            lax.fori_loop(0, ref.shape[0] // 16, piece, 0)

        def s1(p):
            for j, r in enumerate(ORDER):
                for k in (0, 1):
                    for i, d in enumerate((1, -1)):
                        send(1, ("g1", p, j), g(p, k, r, 2, i), R1[p].at[k, i, j],
                             big_dev(k, d))

        def s2(p, j):
            r = ORDER[j]
            arrived(("g1", p, j), blocks(G, p, 1))
            for k in (0, 1):
                for i, d in enumerate((1, -1)):
                    add_into(g(p, k, r, d, i), R1[p].at[k, i, j])
            for k in (0, 1):
                for i, d in enumerate((1, -1)):
                    send(1, ("g2", p, j), g(p, k, r, d), R2[p].at[k, i, j], big_dev(k, d))

        def two(p, j):
            arrived(("g2", p, j), blocks(G, p, 2))

        def s3(p):
            two(p, 0)
            for k in (0, 1):
                add_into(g(p, k, 2, 0), R2[p].at[k, 0, 0], R2[p].at[k, 1, 0])
            for k in (0, 1):
                for i, d in enumerate((1, -1)):
                    send(1, ("g3", p), g(p, k, 2, 0, i), R3[p].at[k, i], small_dev(k, d))

        def pre4(p):
            arrived(("g2", p, 1), blocks(G, p, 4))
            for i, d in enumerate((1, -1)):
                for k in (0, 1):
                    add_into(g(p, k, d, 0), R2[p].at[k, 0, 1 + i], R2[p].at[k, 1, 1 + i])

        def s4(p):
            arrived(("g3", p), blocks(G, p, 1))
            for k in (0, 1):
                for i, d in enumerate((1, -1)):
                    add_into(g(p, k, d, 0, i), R3[p].at[k, i])
            for k in (0, 1):
                for i, d in enumerate((1, -1)):
                    send(1, ("g4", p), g(p, k, d, 0), R4[p].at[k, i], small_dev(k, d))

        def keep(p, k, *others):
            own, to = g(p, k, 0, 0), SUM.at[:, lanes(p, k)]

            def piece(m, carry):
                at = pl.ds(pl.multiple_of(m * 16, 16), 16)
                total = own[at, :].astype(F32)
                for other in others:
                    total = total + other[at, :].astype(F32)
                to[at, :] = total
                return carry

            lax.fori_loop(0, rows // 16, piece, 0)

        def partial_of(xo, core):
            start = (turn(x, xo) * 2 + core) * feats
            span = pl.ds(pl.multiple_of(start, feats), feats)

            def piece(m, carry):
                at = pl.ds(pl.multiple_of(m * tile, tile), tile)
                total = 0.0
                for p in (0, 1):
                    lane = slice(base[p], base[p] + 2 * size[p])
                    total = total + dot(D[at, lane], W[span, lane], ((1,), (1,)))
                PD[at, span] = total.astype(BF)
                return carry
            lax.fori_loop(0, 3, piece, 0)

        def pd(xo, core, part=None):
            start = (turn(x, xo) * 2 + core) * feats
            lane = pl.ds(pl.multiple_of(start, feats), feats)
            if part is None:
                return PD.at[:, lane]
            return PD.at[part * halftok : (part + 1) * halftok, lane]

        for o in (0, 1, -1):
            for k in (0, 1):
                forward(0, k, o, o == 0)
        far_arrived(1, 0)
        last_arrived(0)
        for k in (0, 1):
            forward(0, k, 2)
        gate(0)
        far_arrived(1, 1)
        far_arrived(1, -1)
        for k in (0, 1):
            grads(0, k, 2)
        far_arrived(1, 2)
        s1(0)
        for o in (1, -1):
            for k in (0, 1):
                grads(0, k, o)

        for j, o in enumerate((0, 1, -1)):
            for k in (0, 1):
                forward(1, k, o, o == 0)
            s2(0, j)
        last_arrived(1)
        for k in (0, 1):
            forward(1, k, 2)
        gate(1)
        for k in (0, 1):
            grads(1, k, 2)
        s1(1)
        for o in (1, -1):
            for k in (0, 1):
                grads(1, k, o)
        for k in (0, 1):
            grads(0, k, 0)
        s3(0)
        s2(0, 3)
        left(2, XQ.at[:, 0 : 7 * feats])
        for j, r in enumerate(ORDER):
            partial_of(r, 1 - c)
            send(2, "d0", pd(r, 1 - c), E0.at[j], sibling)

        def sibling_sum(j):
            add_into(pd(ORDER[j], c), E0.at[j])

        partial_of(2, c)
        arrived("d0", PD.at[:, 0 : 4 * feats])
        sibling_sum(0)
        for i, d in enumerate((1, -1)):
            send(2, "d1", pd(2, c, i), E1.at[i], x_dev(d))
        for j in (1, 2):
            partial_of(ORDER[j], c)
            sibling_sum(j)
        for j in (0, 1, 2):
            s2(1, j)
        pre4(0)
        partial_of(0, c)
        s4(0)
        arrived("d1", PD.at[:, 0:feats])
        for i, d in enumerate((1, -1)):
            add_into(pd(d, c, i), E1.at[i])
            send(2, "d2", pd(d, c), E2.at[i], x_dev(d))
        for k in (0, 1):
            grads(1, k, 0)
        s3(1)
        s2(1, 3)
        pre4(1)

        stores = []

        def store(src, dst):
            copy = pltpu.make_async_copy(src, dst, load_sem.at[len(stores)])
            copy.start()
            stores.append(copy)

        def finish_dx():
            arrived("d2", PD.at[:, 0 : 2 * feats])
            own = pd(0, c)

            def piece(m, carry):
                at = pl.ds(pl.multiple_of(m * 16, 16), 16)
                total = (own[at, :].astype(F32) + E0[3, at, :].astype(F32)
                         + E2[0, at, :].astype(F32) + E2[1, at, :].astype(F32))
                DX[at, :] = total.astype(BF)
                return carry

            lax.fori_loop(0, tokens // 16, piece, 0)
            store(DX, dx_out)

        def finish_grads(p):
            two(p, 3)
            if p == 0:
                arrived(("g4", p), blocks(G, p, 2))
            for k in (0, 1):
                late = [R4[p].at[k, i] for i in (0, 1)] if p == 0 else []
                keep(p, k, R2[p].at[k, 0, 3], R2[p].at[k, 1, 3], *late)
            at = slice(base[p], base[p] + 3 * size[p])
            store(SUM.at[:, at], sum_out.at[:, at])

        s4(1)
        finish_dx()
        finish_grads(0)
        finish_grads(1)
        left(0, W.at[0 : 15 * rows, :])
        left(1, G.at[0 : 15 * rows, :])
        left(2, PD.at[:, 0 : 7 * feats])
        for copy in stores:
            copy.wait()
        arrived(("g4", 1), blocks(G, 1, 2))

    count = 2 * (1 + 1 + 4 + 1) + 4 + 2 + 1 + 1
    n = [3 * h // 2 for h in size]
    scratch = [
        pltpu.VMEM((width, every), BF),
        pltpu.VMEM((2 * tokens, width), BF),
        pltpu.VMEM((tokens, every), F32),
        pltpu.VMEM((tokens, every), BF),
        pltpu.VMEM((width, every), BF),
        *[pltpu.VMEM((2, 2, SIDE, half, m), BF) for m in n],
        *[pltpu.VMEM((2, 2, SIDE, rows, m), BF) for m in n],
        *[pltpu.VMEM((2, 2, half, m), BF) for m in n],
        pltpu.VMEM((2, 2, rows, n[0]), BF),
        pltpu.VMEM((tokens, width), BF),
        pltpu.VMEM((SIDE, tokens, feats), BF),
        pltpu.VMEM((2, halftok, feats), BF),
        pltpu.VMEM((2, tokens, feats), BF),
        pltpu.VMEM((hidden, rows), BF),
        pltpu.VMEM((rows, every), F32),
        pltpu.VMEM((tokens, feats), BF),
        pltpu.SemaphoreType.DMA((4,)),
        pltpu.SemaphoreType.DMA((3,)),
        pltpu.SemaphoreType.DMA((count,)),
    ]
    return kernel, scratch


def finish_of(rows, hidden):
    size, base = shares(hidden)
    n = 3 * size[1] // 2
    cut = n - size[1]

    def finish(dx_in, sum_in, late_in, dx_out, gate_out, up_out, down_out,
               DX, SUM, LATE, UP, GATE, DOWN, ins, outs):
        first = slice(0, base[1])
        last = slice(base[1], base[1] + 3 * size[1])
        h, at = size[0], base[1]

        def load(group, src, dst):
            pltpu.make_async_copy(src, dst, ins.at[group]).start()

        def store(group, src, dst):
            pltpu.make_async_copy(src, dst, outs.at[group]).start()

        def done(sems, group, like):
            pltpu.make_async_copy(like, like, sems.at[group]).wait()

        load(0, sum_in.at[:, first], SUM.at[:, first])
        load(1, sum_in.at[:, last], SUM.at[:, last])
        load(1, late_in, LATE)
        load(1, dx_in, DX)
        done(ins, 0, SUM.at[:, first])
        store(0, SUM.at[:, 0:h], gate_out.at[:, 0:h])
        store(0, SUM.at[:, h : 2 * h], up_out.at[:, 0:h])
        DOWN[0:h, :] = SUM[:, 2 * h : 3 * h].T
        store(0, DOWN.at[0:h, :], down_out.at[0:h, :])
        done(ins, 1, SUM)
        store(1, DX, dx_out)
        total = [SUM[:, at + k * n : at + (k + 1) * n] + LATE[k, 0].astype(F32) + LATE[k, 1].astype(F32)
                 for k in (0, 1)]
        GATE[...] = total[0][:, 0 : size[1]]
        store(0, GATE, gate_out.at[:, h:hidden])
        UP[:, 0:cut] = total[0][:, size[1] : n]
        UP[:, cut : size[1]] = total[1][:, 0:cut]
        store(0, UP, up_out.at[:, h:hidden])
        DOWN[h:hidden, :] = total[1][:, cut:n].T
        store(0, DOWN.at[h:hidden, :], down_out.at[h:hidden, :])
        done(outs, 1, DX)
        done(outs, 0, SUM)

    return finish


def solution(mesh):
    def on_device(layer_input, out_cotangent, gate_matrix, up_matrix, down_matrix):
        tokens, feats = layer_input.shape
        rows, hidden = gate_matrix.shape
        width = feats * mesh.shape["tp"]
        kernel, scratch = kernel_of(rows, tokens, width, hidden)
        flops = 2 * 8 * tokens * width * hidden
        late = (2, 2, rows, shares(hidden)[0][1] * 3 // 2)
        any_space = pl.BlockSpec(memory_space=pl.ANY)
        dx, sums, lates = pl.pallas_call(
            kernel,
            out_shape=(
                jax.ShapeDtypeStruct((tokens, feats), BF),
                jax.ShapeDtypeStruct((rows, 3 * hidden), F32),
                jax.ShapeDtypeStruct(late, BF),
            ),
            in_specs=[any_space] * 5,
            out_specs=[any_space] * 3,
            scratch_shapes=scratch,
            compiler_params=pltpu.CompilerParams(
                collective_id=0, has_side_effects=True, vmem_limit_bytes=66_000_000),
            cost_estimate=pl.CostEstimate(
                flops=flops, bytes_accessed=4 << 20, transcendentals=tokens * hidden),
        )(layer_input, out_cotangent, gate_matrix, up_matrix, down_matrix)
        return pl.pallas_call(
            finish_of(rows, hidden),
            out_shape=(
                jax.ShapeDtypeStruct((tokens, feats), BF),
                jax.ShapeDtypeStruct((rows, hidden), F32),
                jax.ShapeDtypeStruct((rows, hidden), F32),
                jax.ShapeDtypeStruct((hidden, rows), F32),
            ),
            in_specs=[any_space] * 3,
            out_specs=[any_space] * 4,
            scratch_shapes=[
                pltpu.VMEM((tokens, feats), BF),
                pltpu.VMEM((rows, 3 * hidden), F32),
                pltpu.VMEM(late, BF),
                pltpu.VMEM((rows, shares(hidden)[0][1]), F32),
                pltpu.VMEM((rows, shares(hidden)[0][1]), F32),
                pltpu.VMEM((hidden, rows), F32),
                pltpu.SemaphoreType.DMA((2,)),
                pltpu.SemaphoreType.DMA((2,)),
            ],
        )(dx, sums, lates)

    return jax.shard_map(
        on_device, mesh=mesh,
        in_specs=(P("fs", "tp"), P("fs", "tp"), P("fs", "tp"), P("fs", "tp"), P("tp", "fs")),
        out_specs=(P("fs", "tp"), P("fs", "tp"), P("fs", "tp"), P("tp", "fs")),
        check_vma=False)
```

```python
import jax
import jax.numpy as jnp
from jax import lax
from jax.experimental import pallas as pl
from jax.experimental.pallas import tpu as pltpu
from jax.sharding import PartitionSpec as P

MESH = pl.DeviceIdType.MESH
BF = jnp.bfloat16
F32 = jnp.float32
SIDE = 4
ORDER = (2, 1, -1, 0)


def shares(hidden):
    first = 2 * hidden // 3
    return (first, hidden - first), (0, 3 * first)


def kernel_of(rows, tokens, width, hidden):
    size, base = shares(hidden)
    half = rows // 2
    feats = width // 8
    band = SIDE * rows
    halftok = tokens // 2
    every = 3 * hidden

    def kernel(x_in, q_in, gate_in, up_in, down_in, dx_out, sum_out, late_out,
               W, XQ, ACC, D, G, R1a, R1b, R2a, R2b, R3a, R3b, R4a, PD, E0, E1, E2, DN, SUM, DX,
               load_sem, ss, rs):
        R1, R2, R3, R4 = (R1a, R1b), (R2a, R2b), (R3a, R3b), (R4a, late_out)
        fs, tp = lax.axis_index("fs"), lax.axis_index("tp")
        z, y = fs // SIDE, fs % SIDE
        x, c = tp // 2, tp % 2

        def turn(a, o):
            return (a + (o % SIDE)) % SIDE

        def fs_dev(f):
            return {"fs": f, "tp": tp}

        def tp_dev(t):
            return {"fs": fs, "tp": t}

        def big_dev(k, d):
            return fs_dev(turn(z, d) * SIDE + y) if k == 0 else fs_dev(z * SIDE + turn(y, d))

        def small_dev(k, d):
            return big_dev(1 - k, d)

        sibling = tp_dev(x * 2 + (1 - c))

        def x_dev(d):
            return tp_dev(turn(x, d) * 2 + c)

        barrier = pltpu.get_barrier_semaphore()
        for partner in (big_dev(0, 1), big_dev(0, -1), big_dev(1, 1), big_dev(1, -1),
                        x_dev(1), x_dev(-1), sibling):
            pl.semaphore_signal(barrier, inc=1, device_id=partner, device_id_type=MESH)
        mine = pl.ds(pl.multiple_of(fs * rows, rows), rows)
        my_feats = pl.ds(pl.multiple_of(tp * feats, feats), feats)
        def load(group, src, dst):
            pltpu.make_async_copy(src, dst, load_sem.at[group]).start()

        def loaded(group, like):
            pltpu.make_async_copy(like, like, load_sem.at[group]).wait()

        for p in (0, 1):
            at, h, from_ = base[p], size[p], p * size[0]
            for i, ref in enumerate((gate_in, up_in)):
                load(3 * p, ref.at[:, from_ : from_ + h],
                     W.at[mine, at + i * h : at + (i + 1) * h])
            if p == 0:
                load(1, down_in, DN)
                load(2, x_in, XQ.at[0:tokens, my_feats])
                load(2, q_in, XQ.at[tokens : 2 * tokens, my_feats])

        def turn_down():
            loaded(1, DN)
            turned = DN[...].astype(F32).T.astype(BF)
            for p in (0, 1):
                at, h, from_ = base[p], size[p], p * size[0]
                W[mine, at + 2 * h : at + 3 * h] = turned[:, from_ : from_ + h]

        def meet():
            pl.semaphore_wait(barrier, 7)

        meet()

        slots, again = {}, {}
        for p in (0, 1):
            for j, r in enumerate(ORDER):
                again["g1", p, j] = "a3", p, r
            again["g2", p, 0] = "a4", p
            again["g2", p, 2] = "g2", p, 1
            again["g3", p] = "a1", p
            again["g4", p] = "a2", p
        again["g2", 1, 1] = again["g2", 1, 2] = "a3", 0, ORDER[0]
        again["g2", 1, 3] = "a3", 0, ORDER[1]
        again["d0"] = "x1", 0

        def slot(name):
            name = again.get(name, name)
            if name not in slots:
                slots[name] = len(slots)
            return slots[name]

        def send(group, name, src, dst, dev):
            pltpu.make_async_remote_copy(
                src_ref=src, dst_ref=dst, send_sem=ss.at[group], recv_sem=rs.at[slot(name)],
                device_id=dev, device_id_type=MESH).start()

        def awaited(name, like):
            return pltpu.make_async_remote_copy(
                src_ref=like, dst_ref=like, send_sem=ss.at[0], recv_sem=rs.at[slot(name)],
                device_id=sibling, device_id_type=MESH)

        def arrived(name, like):
            awaited(name, like).wait_recv()

        def left(group, like):
            pltpu.make_async_remote_copy(
                src_ref=like, dst_ref=like, send_sem=ss.at[group], recv_sem=rs.at[0],
                device_id=sibling, device_id_type=MESH).wait_send()

        def block(k, so, bo, part=None):
            zo, yo = (bo, so) if k == 0 else (so, bo)
            start = (turn(z, zo) * SIDE + turn(y, yo)) * rows
            if part is None:
                return pl.ds(pl.multiple_of(start, rows), rows)
            return pl.ds(pl.multiple_of(start + part * half, half), half)

        def lanes(p, k):
            cols = 3 * size[p] // 2
            return slice(base[p] + k * cols, base[p] + (k + 1) * cols)

        def blocks(ref, p, n):
            return ref.at[0 : n * rows, base[p] : base[p] + 3 * size[p]]

        def w(p, k, so, bo, part=None):
            return W.at[block(k, so, bo, part), lanes(p, k)]

        def near(p, k):
            for d in (1, -1):
                send(0, ("a1", p), w(p, k, 0, 0), w(p, k, 0, 0), small_dev(k, d))

        def far(p, r):
            for k in (0, 1):
                for d in (1, -1):
                    send(0, ("a3", p, r), w(p, k, r, 0), w(p, k, r, 0), big_dev(k, d))

        def near_arrived(p):
            arrived(("a1", p), blocks(W, p, 2))
            for k in (0, 1):
                for i, d in enumerate((1, -1)):
                    send(0, ("a2", p), w(p, k, -d, 0, i), w(p, k, -d, 0, i), small_dev(k, d))

        def opposite_arrived(p):
            arrived(("a2", p), blocks(W, p, 1))

        def far_arrived(p, r):
            arrived(("a3", p, r), blocks(W, p, 2))
            for k in (0, 1):
                for i, d in enumerate((1, -1)):
                    send(0, ("a4", p), w(p, k, r, -d, i), w(p, k, r, -d, i), big_dev(k, d))

        def last_arrived(p):
            arrived(("a4", p), blocks(W, p, 4))

        def xq(xo, core, part):
            start = (turn(x, xo) * 2 + core) * feats
            lane = pl.ds(pl.multiple_of(start, feats), feats)
            return XQ.at[part * tokens : (part + 1) * tokens, lane]

        def x_own(i):
            for d in (1, -1):
                part = i if d == 1 else 1 - i
                send(2, ("x1", i), xq(0, c, part), xq(0, c, part), x_dev(d))

        def to_sibling(xo, part):
            send(2, "sib", xq(xo, c, part), xq(xo, c, part), sibling)

        def x_first():
            arrived(("x1", 0), XQ.at[:, 0:feats])
            for i, d in enumerate((1, -1)):
                send(2, "x2", xq(-d, c, i), xq(-d, c, i), x_dev(d))
            for i, d in enumerate((1, -1)):
                to_sibling(-d, i)

        def x_second():
            arrived(("x1", 1), XQ.at[:, 0:feats])
            for i, d in enumerate((1, -1)):
                to_sibling(-d, 1 - i)

        def x_third():
            arrived("x2", XQ.at[:, 0:feats])
            for i in (0, 1):
                to_sibling(2, i)

        def x_last():
            arrived("sib", XQ.at[:, 0 : 4 * feats])

        loaded(0, W.at[mine, 0 : 2 * size[0]])
        near(0, 0)
        turn_down()
        near(0, 1)
        far(0, 0)
        loaded(2, XQ.at[:, my_feats])
        x_own(0)
        x_own(1)
        for part in (0, 1):
            to_sibling(0, part)
        loaded(3, W.at[mine, base[1] : base[1] + 2 * size[1]])
        for k in (0, 1):
            near(1, k)

        near_arrived(0)
        for r in (1, -1):
            far(0, r)
        x_first()
        far_arrived(0, 0)
        near_arrived(1)
        opposite_arrived(0)
        far(0, 2)
        far_arrived(0, 1)
        x_second()
        far_arrived(0, -1)
        far(1, 0)
        x_third()
        far_arrived(0, 2)
        for r in (1, -1):
            far(1, r)
        opposite_arrived(1)
        far(1, 2)
        x_last()

        tile = tokens // 3

        def dot(a, b, dims):
            return lax.dot_general(a, b, (dims, ((), ())), preferred_element_type=F32)

        def put(at, lane, value, first):
            if first:
                ACC[at, lane] = value
            else:
                ACC[at, lane] += value

        def forward(p, k, o, first=False):
            both = lanes(p, k)
            split = base[p] + 2 * size[p]

            def piece(m, carry):
                at = pl.ds(pl.multiple_of(m * tile, tile), tile)
                low = pl.ds(pl.multiple_of(tokens + m * tile, tile), tile)
                if k == 0:
                    span = pl.ds(pl.multiple_of(turn(z, o) * band, band), band)
                    put(at, both, dot(XQ[at, span], W[span, both], ((1,), (0,))), first)
                else:
                    spans = [pl.ds(pl.multiple_of(i * band + turn(y, o) * rows, rows), rows)
                             for i in range(SIDE)]
                    for top, lane in ((at, slice(both.start, split)), (low, slice(split, both.stop))):
                        a = jnp.concatenate([XQ[top, s] for s in spans], axis=1)
                        b = jnp.concatenate([W[s, lane] for s in spans], axis=0)
                        put(at, lane, dot(a, b, ((1,), (0,))), first)
                return carry
            lax.fori_loop(0, 3, piece, 0)

        step = tokens // 24

        def gate(p):
            h = size[p]
            one, two, three, four = (base[p] + i * h for i in range(4))

            def piece(m, carry):
                at = pl.ds(pl.multiple_of(m * step, step), step)
                g = ACC[at, one:two]
                u = ACC[at, two:three]
                e = ACC[at, three:four]
                s = 1.0 / (1.0 + jnp.exp(-g))
                act = g * s
                D[at, one:two] = (e * u * s * (1.0 + g * (1.0 - s))).astype(BF)
                D[at, two:three] = (e * act).astype(BF)
                D[at, three:four] = (act * u).astype(BF)
                return carry

            lax.fori_loop(0, 24, piece, 0)

        def grads(p, k, o):
            both = lanes(p, k)
            split = base[p] + 2 * size[p]

            def piece(n, carry):
                if k == 0:
                    span = pl.ds(pl.multiple_of(turn(z, o) * band + n * 2 * rows, 2 * rows), 2 * rows)
                    G[span, both] = dot(XQ[0:tokens, span], D[:, both], ((0,), (0,))).astype(BF)
                else:
                    spans = [pl.ds(pl.multiple_of((2 * n + i) * band + turn(y, o) * rows, rows), rows)
                             for i in range(2)]
                    for top, lane in ((0, slice(both.start, split)), (tokens, slice(split, both.stop))):
                        a = jnp.concatenate([XQ[top : top + tokens, s] for s in spans], axis=1)
                        r = dot(a, D[:, lane], ((0,), (0,))).astype(BF)
                        for i in range(2):
                            G[spans[i], lane] = r[i * rows : (i + 1) * rows]
                return carry
            lax.fori_loop(0, 2, piece, 0)

        def g(p, k, so, bo, part=None):
            return G.at[block(k, so, bo, part), lanes(p, k)]

        def add_into(ref, *others):
            def piece(m, carry):
                at = pl.ds(pl.multiple_of(m * 16, 16), 16)
                total = ref[at, :].astype(F32)
                for other in others:
                    total = total + other[at, :].astype(F32)
                ref[at, :] = total.astype(BF)
                return carry
            lax.fori_loop(0, ref.shape[0] // 16, piece, 0)

        def s1(p, colours=(0, 1)):
            for j, r in enumerate(ORDER):
                for k in colours:
                    for i, d in enumerate((1, -1)):
                        send(1, ("g1", p, j), g(p, k, r, 2, i), R1[p].at[k, i, j],
                             big_dev(k, d))

        def s2(p, j):
            r = ORDER[j]
            arrived(("g1", p, j), blocks(G, p, 1))
            for k in (0, 1):
                for i, d in enumerate((1, -1)):
                    add_into(g(p, k, r, d, i), R1[p].at[k, i, j])
            for k in (0, 1):
                for i, d in enumerate((1, -1)):
                    send(1, ("g2", p, j), g(p, k, r, d), R2[p].at[k, i, j], big_dev(k, d))

        def two(p, j):
            arrived(("g2", p, j), blocks(G, p, 2))

        def s3(p):
            two(p, 0)
            for k in (0, 1):
                add_into(g(p, k, 2, 0), R2[p].at[k, 0, 0], R2[p].at[k, 1, 0])
            for k in (0, 1):
                for i, d in enumerate((1, -1)):
                    send(1, ("g3", p), g(p, k, 2, 0, i), R3[p].at[k, i], small_dev(k, d))

        def pre4(p):
            arrived(("g2", p, 1), blocks(G, p, 4))
            for i, d in enumerate((1, -1)):
                for k in (0, 1):
                    add_into(g(p, k, d, 0), R2[p].at[k, 0, 1 + i], R2[p].at[k, 1, 1 + i])

        def s4(p):
            arrived(("g3", p), blocks(G, p, 1))
            for k in (0, 1):
                for i, d in enumerate((1, -1)):
                    add_into(g(p, k, d, 0, i), R3[p].at[k, i])
            for k in (0, 1):
                for i, d in enumerate((1, -1)):
                    send(1, ("g4", p), g(p, k, d, 0), R4[p].at[k, i], small_dev(k, d))

        def keep(p, k, *others):
            own, to = g(p, k, 0, 0), SUM.at[:, lanes(p, k)]

            def piece(m, carry):
                at = pl.ds(pl.multiple_of(m * 16, 16), 16)
                total = own[at, :].astype(F32)
                for other in others:
                    total = total + other[at, :].astype(F32)
                to[at, :] = total
                return carry

            lax.fori_loop(0, rows // 16, piece, 0)

        def partial_of(xo, core):
            start = (turn(x, xo) * 2 + core) * feats
            span = pl.ds(pl.multiple_of(start, feats), feats)

            def piece(m, carry):
                at = pl.ds(pl.multiple_of(m * tile, tile), tile)
                total = 0.0
                for p in (0, 1):
                    lane = slice(base[p], base[p] + 2 * size[p])
                    total = total + dot(D[at, lane], W[span, lane], ((1,), (1,)))
                PD[at, span] = total.astype(BF)
                return carry
            lax.fori_loop(0, 3, piece, 0)

        def pd(xo, core, part=None):
            start = (turn(x, xo) * 2 + core) * feats
            lane = pl.ds(pl.multiple_of(start, feats), feats)
            if part is None:
                return PD.at[:, lane]
            return PD.at[part * halftok : (part + 1) * halftok, lane]

        for o in (0, 1, -1):
            for k in (0, 1):
                forward(0, k, o, o == 0)
        far_arrived(1, 0)
        last_arrived(0)
        for k in (0, 1):
            forward(0, k, 2)
        gate(0)
        far_arrived(1, 1)
        far_arrived(1, -1)
        for k in (0, 1):
            grads(0, k, 2)
        far_arrived(1, 2)
        s1(0)
        for o in (1, -1):
            for k in (0, 1):
                grads(0, k, o)

        for j, o in enumerate((0, 1, -1)):
            for k in (0, 1):
                forward(1, k, o, o == 0)
            s2(0, j)
        last_arrived(1)
        for k in (0, 1):
            forward(1, k, 2)
        gate(1)
        for k in (0, 1):
            grads(1, k, 2)
            s1(1, (k,))
        for o in (1, -1):
            for k in (0, 1):
                grads(1, k, o)
        for k in (0, 1):
            grads(0, k, 0)
        s3(0)
        s2(0, 3)
        left(2, XQ.at[:, 0 : 7 * feats])
        for j, r in enumerate(ORDER):
            partial_of(r, 1 - c)
            send(2, "d0", pd(r, 1 - c), E0.at[j], sibling)

        def sibling_sum(j):
            add_into(pd(ORDER[j], c), E0.at[j])

        partial_of(2, c)
        arrived("d0", PD.at[:, 0 : 4 * feats])
        sibling_sum(0)
        for i, d in enumerate((1, -1)):
            send(2, "d1", pd(2, c, i), E1.at[i], x_dev(d))
        for j in (1, 2):
            partial_of(ORDER[j], c)
            sibling_sum(j)
        for j in (0, 1, 2):
            s2(1, j)
        pre4(0)
        partial_of(0, c)
        s4(0)
        arrived("d1", PD.at[:, 0:feats])
        for i, d in enumerate((1, -1)):
            add_into(pd(d, c, i), E1.at[i])
            send(2, "d2", pd(d, c), E2.at[i], x_dev(d))
        for k in (0, 1):
            grads(1, k, 0)
        s3(1)
        s2(1, 3)
        pre4(1)

        stores = []

        def store(src, dst):
            copy = pltpu.make_async_copy(src, dst, load_sem.at[len(stores)])
            copy.start()
            stores.append(copy)

        def finish_dx():
            arrived("d2", PD.at[:, 0 : 2 * feats])
            own = pd(0, c)

            def piece(m, carry):
                at = pl.ds(pl.multiple_of(m * 16, 16), 16)
                total = (own[at, :].astype(F32) + E0[3, at, :].astype(F32)
                         + E2[0, at, :].astype(F32) + E2[1, at, :].astype(F32))
                DX[at, :] = total.astype(BF)
                return carry

            lax.fori_loop(0, tokens // 16, piece, 0)
            store(DX, dx_out)

        def finish_grads(p):
            two(p, 3)
            if p == 0:
                arrived(("g4", p), blocks(G, p, 2))
            for k in (0, 1):
                late = [R4[p].at[k, i] for i in (0, 1)] if p == 0 else []
                keep(p, k, R2[p].at[k, 0, 3], R2[p].at[k, 1, 3], *late)
            at = slice(base[p], base[p] + 3 * size[p])
            store(SUM.at[:, at], sum_out.at[:, at])

        s4(1)
        finish_dx()
        finish_grads(0)
        finish_grads(1)
        left(0, W.at[0 : 15 * rows, :])
        left(1, G.at[0 : 15 * rows, :])
        left(2, PD.at[:, 0 : 7 * feats])
        for copy in stores:
            copy.wait()
        arrived(("g4", 1), blocks(G, 1, 2))

    count = 2 * (1 + 1 + 4 + 1) + 4 + 2 + 1 + 1
    n = [3 * h // 2 for h in size]
    scratch = [
        pltpu.VMEM((width, every), BF),
        pltpu.VMEM((2 * tokens, width), BF),
        pltpu.VMEM((tokens, every), F32),
        pltpu.VMEM((tokens, every), BF),
        pltpu.VMEM((width, every), BF),
        *[pltpu.VMEM((2, 2, SIDE, half, m), BF) for m in n],
        *[pltpu.VMEM((2, 2, SIDE, rows, m), BF) for m in n],
        *[pltpu.VMEM((2, 2, half, m), BF) for m in n],
        pltpu.VMEM((2, 2, rows, n[0]), BF),
        pltpu.VMEM((tokens, width), BF),
        pltpu.VMEM((SIDE, tokens, feats), BF),
        pltpu.VMEM((2, halftok, feats), BF),
        pltpu.VMEM((2, tokens, feats), BF),
        pltpu.VMEM((hidden, rows), BF),
        pltpu.VMEM((rows, every), F32),
        pltpu.VMEM((tokens, feats), BF),
        pltpu.SemaphoreType.DMA((4,)),
        pltpu.SemaphoreType.DMA((3,)),
        pltpu.SemaphoreType.DMA((count,)),
    ]
    return kernel, scratch


def finish_of(rows, hidden):
    size, base = shares(hidden)
    n = 3 * size[1] // 2
    cut = n - size[1]

    def finish(dx_in, sum_in, late_in, dx_out, gate_out, up_out, down_out,
               DX, SUM, LATE, UP, GATE, DOWN, ins, outs):
        first = slice(0, base[1])
        last = slice(base[1], base[1] + 3 * size[1])
        h, at = size[0], base[1]

        def load(group, src, dst):
            pltpu.make_async_copy(src, dst, ins.at[group]).start()

        def store(group, src, dst):
            pltpu.make_async_copy(src, dst, outs.at[group]).start()

        def done(sems, group, like):
            pltpu.make_async_copy(like, like, sems.at[group]).wait()

        load(0, sum_in.at[:, first], SUM.at[:, first])
        load(1, sum_in.at[:, last], SUM.at[:, last])
        load(1, late_in, LATE)
        load(1, dx_in, DX)
        done(ins, 0, SUM.at[:, first])
        store(0, SUM.at[:, 0:h], gate_out.at[:, 0:h])
        store(0, SUM.at[:, h : 2 * h], up_out.at[:, 0:h])
        DOWN[0:h, :] = SUM[:, 2 * h : 3 * h].T
        store(0, DOWN.at[0:h, :], down_out.at[0:h, :])
        done(ins, 1, SUM)
        store(1, DX, dx_out)
        total = [SUM[:, at + k * n : at + (k + 1) * n] + LATE[k, 0].astype(F32) + LATE[k, 1].astype(F32)
                 for k in (0, 1)]
        GATE[...] = total[0][:, 0 : size[1]]
        store(0, GATE, gate_out.at[:, h:hidden])
        UP[:, 0:cut] = total[0][:, size[1] : n]
        UP[:, cut : size[1]] = total[1][:, 0:cut]
        store(0, UP, up_out.at[:, h:hidden])
        DOWN[h:hidden, :] = total[1][:, cut:n].T
        store(0, DOWN.at[h:hidden, :], down_out.at[h:hidden, :])
        done(outs, 1, DX)
        done(outs, 0, SUM)

    return finish


def solution(mesh):
    def on_device(layer_input, out_cotangent, gate_matrix, up_matrix, down_matrix):
        tokens, feats = layer_input.shape
        rows, hidden = gate_matrix.shape
        width = feats * mesh.shape["tp"]
        kernel, scratch = kernel_of(rows, tokens, width, hidden)
        flops = 2 * 8 * tokens * width * hidden
        late = (2, 2, rows, shares(hidden)[0][1] * 3 // 2)
        any_space = pl.BlockSpec(memory_space=pl.ANY)
        dx, sums, lates = pl.pallas_call(
            kernel,
            out_shape=(
                jax.ShapeDtypeStruct((tokens, feats), BF),
                jax.ShapeDtypeStruct((rows, 3 * hidden), F32),
                jax.ShapeDtypeStruct(late, BF),
            ),
            in_specs=[any_space] * 5,
            out_specs=[any_space] * 3,
            scratch_shapes=scratch,
            compiler_params=pltpu.CompilerParams(
                collective_id=0, has_side_effects=True, vmem_limit_bytes=66_000_000),
            cost_estimate=pl.CostEstimate(
                flops=flops, bytes_accessed=4 << 20, transcendentals=tokens * hidden),
        )(layer_input, out_cotangent, gate_matrix, up_matrix, down_matrix)
        return pl.pallas_call(
            finish_of(rows, hidden),
            out_shape=(
                jax.ShapeDtypeStruct((tokens, feats), BF),
                jax.ShapeDtypeStruct((rows, hidden), F32),
                jax.ShapeDtypeStruct((rows, hidden), F32),
                jax.ShapeDtypeStruct((hidden, rows), F32),
            ),
            in_specs=[any_space] * 3,
            out_specs=[any_space] * 4,
            scratch_shapes=[
                pltpu.VMEM((tokens, feats), BF),
                pltpu.VMEM((rows, 3 * hidden), F32),
                pltpu.VMEM(late, BF),
                pltpu.VMEM((rows, shares(hidden)[0][1]), F32),
                pltpu.VMEM((rows, shares(hidden)[0][1]), F32),
                pltpu.VMEM((hidden, rows), F32),
                pltpu.SemaphoreType.DMA((2,)),
                pltpu.SemaphoreType.DMA((2,)),
            ],
        )(dx, sums, lates)

    return jax.shard_map(
        on_device, mesh=mesh,
        in_specs=(P("fs", "tp"), P("fs", "tp"), P("fs", "tp"), P("fs", "tp"), P("tp", "fs")),
        out_specs=(P("fs", "tp"), P("fs", "tp"), P("fs", "tp"), P("tp", "fs")),
        check_vma=False)
```
